512 devices in a mesh: sp: 32 (over z, core), tp: 16 (over y, x).
Axes of the slice: x: 4, y: 4, z: 16, core: 2. Of those that a mesh axis runs over, the one named last changes fastest.
Arguments:
- stream: bfloat16 [2048, 4096], P('tp', 'sp')
- values_in: bfloat16 [1024, 4096], P('tp', 'sp'), may hold values from -6 to 6
- in_gate: bfloat16 [1024, 4096], P('tp', 'sp'), may hold values from -6 to 6
- out_gate: bfloat16 [1024, 4096], P('tp', 'sp'), may hold values from -6 to 6
- documents: int32 [4096], P('sp'), may hold values from 0 to 63, never falling along the last dimension, each value on 1 to 256 neighbouring positions
- conv_taps: float32 [3, 1024], P(None, 'tp'), may hold values from -3.5 to 3.5
- head_gain: float32 [1024], P('tp'), may hold values from 0.1 to 1.9
- mix_weight: bfloat16 [1024, 2048], P('tp'), may hold values from -0.25 to 0.25
- norm_gain: float32 [2048], P('tp'), may hold values from 0.1 to 1.9
- routes: int32 [4096, 4], P('sp'), may hold values from 0 to 31, all different within a row; in each aligned block of 128 rows (0 to 127, 128 to 255, ...) at most 24 rows name the same one
- route_weight: float32 [4096, 4], P('sp'), may hold values from 0.2 to 1
- expert_gate: bfloat16 [32, 2048, 2048], P('sp', None, 'tp'), may hold values from -0.125 to 0.125
- expert_up: bfloat16 [32, 2048, 2048], P('sp', None, 'tp'), may hold values from -0.125 to 0.125
- expert_down: bfloat16 [32, 2048, 2048], P('sp', None, 'tp'), may hold values from -0.125 to 0.125
- shared_gate: bfloat16 [2048, 2048], P(None, 'tp'), may hold values from -0.125 to 0.125
- shared_up: bfloat16 [2048, 2048], P(None, 'tp'), may hold values from -0.125 to 0.125
- shared_down: bfloat16 [2048, 2048], P('tp'), may hold values from -0.1875 to 0.1875
Outputs:
- layer_out: bfloat16 [2048, 4096], P('tp', 'sp')
The draws below stay inside these ranges and needn't reach their ends.
Inputs may be any that keep to these rules, and one draw needn't show every extreme that they name: `routes`: each row names 4 different experts. In each aligned block of 128 rows no expert is named by more than 24 rows, a bound that some block reaches. `documents`: document numbers never fall along the positions; each document has 1 to 256 positions, and one has exactly that many.
All inputs are finite; a program needn't handle non-finite values.
Results may differ from the reference program's by a relative error of at most 0.015.
Values may be sent and summed in bfloat16 or wider, within the bound.
A program may use at most 64 MiB of HBM per device.

```python
import math
import jax
import jax.numpy as jnp
import numpy as np
from jax import lax

D = 2048
HEADS = 16
HEAD = 64
CW = 1024
FE = 2048
FS = 2048
TOP_K = 4
TOK_DEV = 128
TOKENS = 4096
EXPERTS = 32
CAP = 24
N_SP = 32
N_TP = 16


def draw_stream(key, part):
    first = jax.random.fold_in(jax.random.fold_in(key, 11), 0)
    feature_scale = 0.5 * 4.0 ** (jnp.arange(D, dtype=jnp.float32) / D)
    base = jax.random.normal(first, (D, TOKENS), jnp.float32)
    return (base * feature_scale[:, None]).astype(jnp.bfloat16)


def with_spikes(entries, key, source, target, blocks, factor):
    owner, partner = [(jnp.arange(entries.shape[position]) // (entries.shape[position] // blocks)).reshape([-1 if axis == position else 1 for axis in range(entries.ndim)]) for position in (source, target)]
    chosen = jax.random.permutation(key, blocks)[partner]
    strong = (owner == chosen) | (owner == (partner + blocks // 2) % blocks)
    return jnp.where(strong, factor * entries, entries)


def steps_of(own_key, shape, pieces, low, high):
    factor_of = 1.0
    for dim, blocks in pieces:
        heights = jax.random.uniform(jax.random.fold_in(jax.random.fold_in(own_key, 6), dim), (blocks,), jnp.float32, low / len(pieces), high / len(pieces))
        factor_of = factor_of * jnp.repeat(jnp.exp(heights), shape[dim] // blocks).reshape((-1,) + (1,) * (len(shape) - 1 - dim))
    return factor_of


def profile(number_of, total, reach, slope):
    weights = [(1 << 20) // math.isqrt(rank ** slope) + 1 for rank in range(2, number_of + 1)]
    spare, counts = total - reach - (number_of - 1), [1] * (number_of - 1)
    while spare > 0:
        free = [i for i in range(number_of - 1) if counts[i] < reach]
        pool, budget = sum([weights[i] for i in free]), spare
        for i in free:
            addition = min(reach - counts[i], max(1, budget * weights[i] // pool), spare)
            counts[i] = counts[i] + addition
            spare = spare - addition
    return np.array([reach] + counts)


def uneven_parts(own_key, number_of, total, most, lean):
    if number_of == 2:
        one = jax.random.randint(own_key, (), max(1, total - most), min(most, total - 1) + 1)
        return jnp.stack([one, total - one])
    lengths = jnp.asarray(profile(number_of, total, most, lean), jnp.int32)
    twos = (number_of - 1) // 2
    donor, receiver = lengths[1:1 + 2 * twos:2], lengths[2:2 + 2 * twos:2]
    room = jnp.minimum(donor - 1, most - receiver)
    passed = jax.random.randint(jax.random.fold_in(own_key, 1), (twos,), 0, 1 << 20) % (room + 1)
    lengths = lengths.at[1:1 + 2 * twos:2].set(donor - passed).at[2:2 + 2 * twos:2].set(receiver + passed)
    return lengths[jax.random.permutation(jax.random.fold_in(own_key, 2), number_of)]


def deal_out(stream_key, own, number, rows, amount, top, reach, lean):
    ranking = jax.random.permutation(stream_key, amount)
    heavy_load, usual = portions_of(amount, rows * top, reach, lean, True), portions_of(amount, rows * top, reach, lean, False)
    places = jnp.arange(amount)

    def named(lengths, turn):
        used = int((lengths > 0).sum())
        fixed = max(1, used // 4)
        passed = fixed + (places - fixed + turn * (used - fixed)) % max(1, amount - fixed)
        return jnp.zeros((amount,), jnp.int32).at[ranking[jnp.where(places < fixed, places, passed)]].set(jnp.asarray(lengths, jnp.int32))

    lengths = jnp.where(number % 4 == 0, named(heavy_load, number // 4), named(usual, number - number // 4 - 1))
    mixed = jax.random.permutation(jax.random.fold_in(own, 3), amount)
    source_of, taker = mixed[0:amount // 2 * 2:2], mixed[1:amount // 2 * 2:2]
    room = jnp.minimum(lengths[source_of] - 1, reach - lengths[taker]) // 2
    room = jnp.where((source_of == ranking[0]) | (taker == ranking[0]) | (lengths[taker] == 0), 0, jnp.maximum(room, 0))
    passed = jax.random.randint(jax.random.fold_in(own, 4), (amount // 2,), 0, 1 << 20) % (room + 1)
    lengths = lengths.at[source_of].add(-passed).at[taker].add(passed)
    items = jnp.searchsorted(jnp.cumsum(lengths), jnp.arange(rows * top), side="right").astype(jnp.int32)
    listing = items.reshape(top, rows).T
    listing = listing[jax.random.permutation(jax.random.fold_in(own, 1), rows)]
    turn = jax.random.randint(jax.random.fold_in(own, 2), (rows, 1), 0, top)
    return jnp.take_along_axis(listing, (jnp.arange(top)[None, :] + turn) % top, axis=1)


def portions_of(amount, total, bound, skew, full):
    loads = [(1 << 20) // math.isqrt(standing ** skew) + 1 for standing in range(1, amount + 1)]
    largest = bound if full else min(bound, max(-(-total // amount), total * loads[0] // sum(loads)))
    least = 1 if total - largest >= amount - 1 else 0
    given, rest = [largest] + [least] * (amount - 1), total - largest - least * (amount - 1)
    while rest > 0:
        movable = [i for i in range(1, amount) if given[i] < largest] or [i for i in range(1, amount) if given[i] < bound]
        mass, budget = sum([loads[i] for i in movable]), rest
        for i in movable:
            more = min(bound - given[i], max(1, budget * loads[i] // mass), rest)
            given[i] = given[i] + more
            rest = rest - more
    return np.array(given)


def noise(own_key, extent, scale, bound, cuts=(), kind=jnp.bfloat16):
    array = jax.random.normal(own_key, extent, jnp.float32) * scale
    if len(cuts) > 0:
        array = steps_of(own_key, extent, cuts, -0.22, 0.18) * array
    return jnp.clip(array, min=-bound, max=bound).astype(kind)


def bell_draw_with(own_key, dims, scale, most, cuts, heavy, kind=jnp.bfloat16):
    result = scale * jax.random.normal(own_key, dims, jnp.float32)
    if cuts:
        result = result * steps_of(own_key, dims, cuts, -0.22, 0.18)
    return jnp.clip(with_spikes(result, jax.random.fold_in(own_key, 3), *heavy), -most, most).astype(kind)


def setup_inputs(seed: int = 0) -> dict:
    seeds = jax.random.split(jax.random.key(seed), 18)
    stream = draw_stream(jax.random.fold_in(seeds[17], 71), 0)
    values_in = noise(seeds[1], (CW, TOKENS), 1.0, 6.0, ((0, 16), (1, 32)))
    in_gate = noise(seeds[2], (CW, TOKENS), 1.0, 6.0, ((0, 16), (1, 32)))
    out_gate = noise(seeds[3], (CW, TOKENS), 1.0, 6.0, ((0, 16), (1, 32)))
    documents = jnp.searchsorted(jnp.cumsum(uneven_parts(seeds[4], 2 * N_SP, TOKENS, 2 * TOK_DEV, 1)), jnp.arange(TOKENS), side="right").astype(jnp.int32)
    conv_taps = noise(seeds[5], (3, CW), 3 ** -0.5, 3.5, ((1, 16),), jnp.float32)
    head_gain = jnp.clip(1.0 + 0.18 * jax.random.normal(seeds[6], (CW,), jnp.float32), 0.1, 1.9)
    mix_weight = bell_draw_with(seeds[7], (CW, D), CW ** -0.5, 0.25, ((0, 16),), (0, 1, 16, 2.0))
    norm_gain = jnp.clip(1.0 + 0.18 * jax.random.normal(seeds[8], (D,), jnp.float32), 0.1, 1.9)
    routes_keys = jax.random.split(jax.random.fold_in(seeds[9], 1), TOKENS // TOK_DEV)
    routes_turns = jax.random.permutation(jax.random.fold_in(seeds[9], 3), TOKENS // TOK_DEV)
    routes = jax.vmap(lambda own, number: deal_out(jax.random.fold_in(seeds[9], 2), own, number, TOK_DEV, EXPERTS, TOP_K, CAP, 1))(routes_keys, routes_turns).reshape((TOKENS, TOP_K))
    route_weight = jnp.clip(0.2 + 0.8 * jax.random.uniform(seeds[10], (TOKENS, TOP_K), jnp.float32) ** steps_of(seeds[10], (TOKENS, TOP_K), ((0, 32),), -0.2, 0.2), 0.2, 1.0)
    expert_gate = noise(seeds[11], (EXPERTS, D, FE), D ** -0.5, 0.125, ((0, 32), (2, 16)))
    expert_up = noise(seeds[12], (EXPERTS, D, FE), D ** -0.5, 0.125, ((0, 32), (2, 16)))
    expert_down = noise(seeds[13], (EXPERTS, FE, D), FE ** -0.5, 0.125, ((0, 32), (2, 16)))
    shared_gate = noise(seeds[14], (D, FS), D ** -0.5, 0.125, ((1, 16),))
    shared_up = noise(seeds[15], (D, FS), D ** -0.5, 0.125, ((1, 16),))
    shared_down = bell_draw_with(seeds[16], (FS, D), FS ** -0.5, 0.1875, ((0, 16),), (0, 1, 16, 2.0))
    return {"stream": stream, "values_in": values_in, "in_gate": in_gate, "out_gate": out_gate, "documents": documents, "conv_taps": conv_taps, "head_gain": head_gain, "mix_weight": mix_weight, "norm_gain": norm_gain, "routes": routes, "route_weight": route_weight, "expert_gate": expert_gate, "expert_up": expert_up, "expert_down": expert_down, "shared_gate": shared_gate, "shared_up": shared_up, "shared_down": shared_down}


epsilon = 1e-06

def rounded(value):
    return lax.optimization_barrier(value.astype(jnp.bfloat16)).astype(jnp.float32)

def block_sum(left, right, parts):
    width = left.shape[1] // parts
    running = jnp.zeros((left.shape[0], right.shape[1]), jnp.float32)
    for block in range(parts):
        term = jnp.dot(left[:, block * width:(block + 1) * width], right[block * width:(block + 1) * width], preferred_element_type=jnp.float32)
        running = running + rounded(term)
    return running

def reference(stream, values_in, in_gate, out_gate, documents, conv_taps, head_gain, mix_weight, norm_gain, routes, route_weight, expert_gate, expert_up, expert_down, shared_gate, shared_up, shared_down):
    product = values_in.astype(jnp.float32) * in_gate.astype(jnp.float32)
    length = product.shape[1]
    padded = jnp.pad(product, ((0, 0), (2, 0)))
    doc_ids = jnp.pad(documents, (2, 0), constant_values=-1)
    convolved = jnp.zeros(product.shape, jnp.float32)
    for offset in range(3):
        same_doc = (doc_ids[offset:offset + length] == documents).astype(jnp.float32)
        convolved = convolved + conv_taps[offset][:, None] * padded[:, offset:offset + length] * same_doc[None, :]
    mixed = out_gate.astype(jnp.float32) * convolved
    heads = mixed.reshape(HEADS, HEAD, length)
    heads = heads * lax.rsqrt(lax.optimization_barrier(jnp.mean(heads * heads, axis=1, keepdims=True)) + epsilon)
    normed_heads = (heads.reshape(CW, length) * head_gain[:, None]).astype(jnp.bfloat16)
    mixer = block_sum(normed_heads.T, mix_weight, N_TP)
    hidden_state = stream.astype(jnp.float32).T + mixer
    normed = (hidden_state * lax.rsqrt(lax.optimization_barrier(jnp.mean(hidden_state * hidden_state, axis=1, keepdims=True)) + epsilon) * norm_gain[None, :]).astype(jnp.bfloat16)
    shared_mid = (jax.nn.silu(jnp.dot(normed, shared_gate, preferred_element_type=jnp.float32)) * jnp.dot(normed, shared_up, preferred_element_type=jnp.float32)).astype(jnp.bfloat16)
    shared = block_sum(shared_mid, shared_down, N_TP)
    groups = TOKENS // TOK_DEV
    flat_routes = routes.reshape(groups, TOK_DEV * TOP_K)
    onehot = (flat_routes[:, :, None] == jnp.arange(EXPERTS, dtype=jnp.int32)[None, None, :]).astype(jnp.int32)
    earlier = jnp.cumsum(onehot, axis=1) - onehot
    slot = lax.optimization_barrier(jnp.sum(earlier * onehot, axis=2))
    column = (jnp.arange(groups, dtype=jnp.int32)[:, None] * CAP + slot).reshape(-1).astype(jnp.int32)
    owner = (jnp.arange(TOKENS * TOP_K, dtype=jnp.int32) // TOP_K).astype(jnp.int32)
    chosen = flat_routes.reshape(-1)
    table = jnp.zeros((EXPERTS, groups * CAP), jnp.int32).at[chosen, column].set(owner)
    filled = jnp.zeros((EXPERTS, groups * CAP), jnp.bfloat16).at[chosen, column].set(1.0)

    def expert(number):
        rows = normed[table[number]] * filled[number][:, None]
        gate = jnp.dot(rows, expert_gate[number], preferred_element_type=jnp.float32)
        upward = jnp.dot(rows, expert_up[number], preferred_element_type=jnp.float32)
        middle = (jax.nn.silu(gate) * upward).astype(jnp.bfloat16)
        return jnp.dot(middle, expert_down[number], preferred_element_type=jnp.float32).astype(jnp.bfloat16)
    outputs = lax.map(expert, jnp.arange(EXPERTS, dtype=jnp.int32))
    picked = outputs[chosen, column].astype(jnp.float32).reshape(TOKENS, TOP_K, D)
    routed = lax.optimization_barrier(jnp.sum(picked * route_weight[:, :, None], axis=1))
    return (hidden_state + shared + routed).astype(jnp.bfloat16).T
```

```python
import jax
import jax.numpy as jnp
from jax import lax
from jax.experimental import pallas as pl
from jax.experimental.pallas import tpu as pltpu
from jax.sharding import PartitionSpec as P

F32 = jnp.float32
BF16 = jnp.bfloat16
MESH = pl.DeviceIdType.MESH
EPS = 1e-06

D = 2048
T = 128
HEAD = 64
N_SP = 32
N_TP = 16
N_Z = 16
SIDE = 4
CAP = 24
TOP_K = 4
SLOTS = N_SP * CAP
CHUNKS = 2
PER_CHUNK = N_SP // CHUNKS
HALF = PER_CHUNK // 2
QUARTER = HALF // 2
NEAR = 3


def dot(a, b, contract=((1,), (0,)), precision=None):
    return lax.dot_general(
        a, b, (contract, ((), ())), precision=precision, preferred_element_type=F32
    )


def iota(shape, dim):
    return lax.broadcasted_iota(jnp.int32, shape, dim)


def column_of(row, n):
    eye = iota((n, n), 0) == iota((n, n), 1)
    return jnp.sum(jnp.where(eye, jnp.broadcast_to(row, (n, n)), 0.0), axis=1, keepdims=True)


def kernel(
    stream,
    values_in,
    in_gate,
    out_gate,
    documents,
    conv_taps,
    head_gain,
    mix_weight,
    norm_gain,
    routes,
    route_weight,
    expert_gate,
    expert_up,
    expert_down,
    shared_gate,
    shared_up,
    shared_down,
    out,
    halo_v,
    halo_g,
    halo_d,
    mix_w,
    w_gu,
    w_down,
    s_gu,
    s_down,
    mix_part,
    mix_in,
    sq_out,
    sq_in,
    normed_all,
    pick,
    comb_hi,
    comb_lo,
    disp_out,
    rows_all,
    mid_all,
    ret_out,
    ret_in,
    sh_part,
    sh_in,
    hidden,
    load_sem,
    halo_s,
    halo_r,
    mix_s,
    mix_r,
    sq_s,
    sq_r,
    nrm_s,
    nrm_r,
    disp_s,
    disp_r,
    gat_s,
    gat_r,
    ret_s,
    ret_r,
    sh_s,
    sh_r,
):
    sp = lax.axis_index("sp")
    tp = lax.axis_index("tp")
    z, core = sp // 2, sp % 2
    y, x = tp // SIDE, tp % SIDE

    def remote(src, dst, send, recv, **where):
        return pltpu.make_async_remote_copy(
            src_ref=src,
            dst_ref=dst,
            send_sem=send,
            recv_sem=recv,
            device_id=where,
            device_id_type=MESH,
        )

    barrier = pltpu.get_barrier_semaphore()

    @pl.loop(1, N_SP)
    def _(step):
        pl.semaphore_signal(
            barrier, inc=1, device_id={"sp": (sp + step) % N_SP}, device_id_type=MESH
        )

    @pl.loop(1, N_TP)
    def _(step):
        pl.semaphore_signal(
            barrier, inc=1, device_id={"tp": (tp + step) % N_TP}, device_id_type=MESH
        )

    loads = [
        pltpu.make_async_copy(src, dst, load_sem.at[i])
        for i, (src, dst) in enumerate(
            [
                (mix_weight, mix_w),
                (shared_gate, s_gu.at[:, pl.ds(0, T)]),
                (shared_up, s_gu.at[:, pl.ds(T, T)]),
                (shared_down, s_down),
                (expert_gate.at[0], w_gu.at[:, pl.ds(0, T)]),
                (expert_up.at[0], w_gu.at[:, pl.ds(T, T)]),
                (expert_down.at[0], w_down),
            ]
        )
    ]
    for load in loads:
        load.start()

    lane = iota((T, T), 1)
    named = jnp.zeros((T, T), F32)
    weight = jnp.zeros((T, T), F32)
    for k in range(TOP_K):
        hit = routes[:, k : k + 1] == lane
        named = jnp.where(hit, 1.0, named)
        weight = jnp.where(hit, route_weight[:, k : k + 1], weight)
    before = jnp.where(iota((T, T), 0) > lane, 1.0, 0.0).astype(BF16)
    earlier = dot(before, named.astype(BF16))
    slot = jnp.where(named > 0, earlier, 200.0).astype(BF16)

    def slot_number(shape, dim):
        number = iota(shape, dim).astype(F32)
        return number - CAP * jnp.floor((number + 0.5) * (1.0 / CAP))

    away = iota((SLOTS, T), 0) - CAP * iota((SLOTS, T), 1)
    owner = jnp.where((away >= 0) & (away < CAP), 1.0, 0.0).astype(BF16)
    taken = dot(owner, slot, ((1,), (1,)))
    pick[...] = jnp.where(taken == slot_number((SLOTS, T), 0), 1.0, 0.0).astype(BF16)
    away = iota((T, SLOTS), 1) - CAP * iota((T, SLOTS), 0)
    owner = jnp.where((away >= 0) & (away < CAP), 1.0, 0.0).astype(BF16)
    taken = dot(slot, owner) == slot_number((T, SLOTS), 1)
    weight_hi = weight.astype(BF16)
    weight_lo = (weight - weight_hi.astype(F32)).astype(BF16)
    comb_hi[...] = jnp.where(taken, dot(weight_hi, owner), 0.0).astype(BF16)
    comb_lo[...] = jnp.where(taken, dot(weight_lo, owner), 0.0).astype(BF16)

    pl.semaphore_wait(barrier, N_SP + N_TP - 2)

    behind = (sp + 1) % N_SP
    halos = [
        remote(src, dst, halo_s.at[i], halo_r.at[i], sp=behind)
        for i, (src, dst) in enumerate(
            [(values_in, halo_v), (in_gate, halo_g), (documents, halo_d)]
        )
    ]
    for halo in halos:
        halo.start()
    product = values_in[...].astype(F32) * in_gate[...].astype(F32)
    docs = jnp.broadcast_to(documents[...], (8, T))
    tap = [column_of(conv_taps[j : j + 1, :], HEAD) for j in range(3)]
    gain_col = column_of(head_gain[...], HEAD)
    for halo in halos:
        halo.wait_recv()
    product_before = halo_v[...].astype(F32) * halo_g[...].astype(F32)
    docs_before = jnp.where(sp == 0, -1, jnp.broadcast_to(halo_d[...], (8, T)))
    convolved = jnp.zeros((HEAD, T), F32)
    for j in range(3):
        back = 2 - j
        if back:
            shifted = jnp.where(
                iota((HEAD, T), 1) < back,
                pltpu.roll(product_before, back, 1),
                pltpu.roll(product, back, 1),
            )
            docs_then = jnp.where(
                iota((8, T), 1) < back,
                pltpu.roll(docs_before, back, 1),
                pltpu.roll(docs, back, 1),
            )
            same = jnp.where(docs_then == docs, 1.0, 0.0)[0:1, :]
            convolved = convolved + tap[j] * shifted * same
        else:
            convolved = convolved + tap[j] * product
    mixed = out_gate[...].astype(F32) * convolved
    spread = jnp.mean(mixed * mixed, axis=0, keepdims=True)
    heads = (mixed * lax.rsqrt(spread + EPS) * gain_col).T.astype(BF16)

    loads[0].wait()
    for j in range(N_TP // 2):
        part = dot(heads, mix_w[:, 2 * T * j : 2 * T * (j + 1)]).astype(BF16)
        mix_part[2 * j] = part[:, :T]
        mix_part[2 * j + 1] = part[:, T:]

    def to_plane(src_of, dst, send, recv):
        def copy(step):
            peer = (tp + step) % N_TP
            return remote(src_of(peer), dst.at[tp], send.at[step], recv.at[step], tp=peer)

        return copy

    def start_plane(copy):
        @pl.loop(1, N_TP)
        def _(step):
            copy(step).start()

    def wait_plane(copy):
        @pl.loop(1, N_TP)
        def _(step):
            copy(step).wait_recv()

    mix_copy = to_plane(lambda peer: mix_part.at[peer], mix_in, mix_s, mix_r)
    start_plane(mix_copy)
    mix_in[tp] = mix_part[tp]
    total = stream[...].astype(F32).T
    wait_plane(mix_copy)
    for j in range(N_TP):
        total = total + mix_in[j].astype(F32)
    hidden[...] = total

    squares = dot(jnp.ones((8, T), F32), total * total, ((1,), (1,)), lax.Precision.HIGHEST)
    sq_out[...] = squares
    sq_copy = to_plane(lambda peer: sq_out, sq_in, sq_s, sq_r)
    start_plane(sq_copy)
    sq_in[tp] = squares
    wait_plane(sq_copy)
    squares = sq_in[0]
    for j in range(1, N_TP):
        squares = squares + sq_in[j]
    scale = column_of(lax.rsqrt(squares / D + EPS)[0:1, :], T)
    normed = (hidden[...] * scale * norm_gain[...]).astype(BF16)

    normed_all[tp] = normed
    disp_out[...] = dot(pick[...], normed).astype(BF16).reshape(N_SP, CAP, T)
    shifts = [0] + [s for d in range(1, 8) for s in (d, -d)] + [8]
    order = [(dz, other) for dz in shifts for other in (0, 1)][1:]

    def disp_copy(dz, other):
        place = (dz + NEAR) % N_Z
        expert = 2 * ((z - dz + N_Z) % N_Z) + ((core + 1 + other) % 2 if dz else 1 - core)
        block = 2 * place + core
        return remote(
            disp_out.at[expert],
            rows_all.at[y, x, block],
            disp_s.at[2 * place + other],
            disp_r.at[block],
            sp=expert,
        )

    def arrived(dz, other):
        place = (dz + NEAR) % N_Z
        return 2 * place + (other if dz else 1 - core)

    for dz, other in order:
        disp_copy(dz, other).start()
    own = 2 * NEAR + core
    rows_all[y, x, own] = disp_out[sp]

    nrm_copy = to_plane(lambda peer: normed_all.at[tp], normed_all, nrm_s, nrm_r)
    start_plane(nrm_copy)

    def wait_disp(chunk):
        for dz, other in order:
            if ((dz + NEAR) % N_Z) // (N_Z // CHUNKS) == chunk:
                block = arrived(dz, other)
                remote(
                    disp_out.at[0], rows_all.at[y, x, block], disp_s.at[0], disp_r.at[block], sp=behind
                ).wait_recv()

    def tp_at(axis, way):
        if axis == 0:
            return SIDE * y + (x + way + SIDE) % SIDE
        return SIDE * ((y + way + SIDE) % SIDE) + x

    def gather_copies(buf, which, chunk, step):
        copies = []
        for half in range(2):
            start = PER_CHUNK * chunk + HALF * half
            axis = half if step < 2 else 1 - half
            for way in (1, -1):
                quarter = pl.ds(start if way > 0 else start + QUARTER, QUARTER)
                whole = pl.ds(start, HALF)
                from_x = (x - way + SIDE) % SIDE
                from_y = (y - way + SIDE) % SIDE
                if step == 0:
                    ref = buf.at[y, x, whole]
                elif step == 1:
                    ref = buf.at[y, from_x, quarter] if axis == 0 else buf.at[from_y, x, quarter]
                elif step == 2:
                    ref = buf.at[:, x, whole] if axis == 0 else buf.at[y, :, whole]
                else:
                    ref = buf.at[:, from_x, quarter] if axis == 0 else buf.at[from_y, :, quarter]
                index = (((which * CHUNKS + chunk) * 4 + step) * 2 + half) * 2 + (way > 0)
                copies.append(
                    remote(ref, ref, gat_s.at[index], gat_r.at[index], tp=tp_at(axis, way))
                )
        return copies

    bufs = (rows_all, mid_all)

    def go(which, chunk, step):
        for copy in gather_copies(bufs[which], which, chunk, step):
            copy.start()

    def got(which, chunk, step):
        for copy in gather_copies(bufs[which], which, chunk, step):
            copy.wait_recv()

    def gathered(buf, chunk):
        part = pl.ds(PER_CHUNK * chunk, PER_CHUNK)
        return jnp.concatenate(
            [
                buf[i, j, part].reshape(PER_CHUNK * CAP, T)
                for i in range(SIDE)
                for j in range(SIDE)
            ],
            axis=1,
        )

    def silu(v):
        return v / (1.0 + jnp.exp(-v))

    def gate_up(chunk):
        both = dot(gathered(rows_all, chunk), w_gu[...])
        mid = (silu(both[:, :T]) * both[:, T:]).astype(BF16)
        mid_all[y, x, pl.ds(PER_CHUNK * chunk, PER_CHUNK)] = mid.reshape(PER_CHUNK, CAP, T)

    def down(chunk):
        result = dot(gathered(mid_all, chunk), w_down[...]).astype(BF16)
        ret_out[pl.ds(PER_CHUNK * chunk, PER_CHUNK)] = result.reshape(PER_CHUNK, CAP, T)

    def ret_copy(dz, other):
        place = (dz + NEAR) % N_Z
        group_core = (core + 1 + other) % 2 if dz else 1 - core
        group = 2 * ((z + dz + N_Z) % N_Z) + group_core
        return remote(
            ret_out.at[2 * place + group_core],
            ret_in.at[sp],
            ret_s.at[2 * place + other],
            ret_r.at[2 * place + core],
            sp=group,
        )

    def start_ret(chunk):
        for dz, other in order[::-1]:
            if ((dz + NEAR) % N_Z) // (N_Z // CHUNKS) == chunk:
                ret_copy(dz, other).start()

    def shared_expert():
        for load in loads[1:4]:
            load.wait()
        everything = jnp.concatenate([normed_all[j] for j in range(N_TP)], axis=1)
        both = dot(everything, s_gu[...])
        mid = (silu(both[:, :T]) * both[:, T:]).astype(BF16)
        for j in range(N_TP // 2):
            part = dot(mid, s_down[:, 2 * T * j : 2 * T * (j + 1)]).astype(BF16)
            sh_part[2 * j] = part[:, :T]
            sh_part[2 * j + 1] = part[:, T:]

    sh_copy = to_plane(lambda peer: sh_part.at[peer], sh_in, sh_s, sh_r)

    wait_disp(0)
    go(0, 0, 0)
    got(0, 0, 0)
    go(0, 0, 1)
    wait_plane(nrm_copy)
    shared_expert()
    sh_in[tp] = sh_part[tp]
    got(0, 0, 1)
    go(0, 0, 2)
    wait_disp(1)
    go(0, 1, 0)
    got(0, 1, 0)
    go(0, 1, 1)
    got(0, 0, 2)
    go(0, 0, 3)
    got(0, 1, 1)
    go(0, 1, 2)
    for load in loads[4:]:
        load.wait()
    got(0, 0, 3)
    gate_up(0)
    go(1, 0, 0)
    got(0, 1, 2)
    go(0, 1, 3)
    got(1, 0, 0)
    go(1, 0, 1)
    got(0, 1, 3)
    gate_up(1)
    go(1, 1, 0)
    got(1, 0, 1)
    go(1, 0, 2)
    got(1, 1, 0)
    go(1, 1, 1)
    got(1, 0, 2)
    go(1, 0, 3)
    got(1, 1, 1)
    go(1, 1, 2)
    got(1, 0, 3)
    down(0)
    start_ret(0)
    ret_in[sp] = ret_out[own]
    got(1, 1, 2)
    go(1, 1, 3)
    start_plane(sh_copy)
    got(1, 1, 3)
    down(1)
    start_ret(1)

    wait_plane(sh_copy)
    total = hidden[...]
    for j in range(N_TP):
        total = total + sh_in[j].astype(F32)
    for dz, other in order:
        block = arrived(dz, other)
        remote(ret_out.at[0], ret_in.at[0], ret_s.at[0], ret_r.at[block], sp=behind).wait_recv()
    returned = ret_in[...].reshape(SLOTS, T)
    total = total + dot(comb_hi[...], returned) + dot(comb_lo[...], returned)
    out[...] = total.T.astype(BF16)

    for halo in halos:
        halo.wait_send()
    for copy in (mix_copy, sq_copy, nrm_copy, sh_copy):

        @pl.loop(1, N_TP)
        def _(step, copy=copy):
            copy(step).wait_send()

    for dz, other in order:
        disp_copy(dz, other).wait_send()
        ret_copy(dz, other).wait_send()
    for which in range(2):
        for chunk in range(CHUNKS):
            for step in range(4):
                for copy in gather_copies(bufs[which], which, chunk, step):
                    copy.wait_send()


def local(
    stream,
    values_in,
    in_gate,
    out_gate,
    documents,
    conv_taps,
    head_gain,
    mix_weight,
    norm_gain,
    routes,
    route_weight,
    expert_gate,
    expert_up,
    expert_down,
    shared_gate,
    shared_up,
    shared_down,
):
    vmem = pl.BlockSpec(memory_space=pltpu.VMEM)
    hbm = pl.BlockSpec(memory_space=pl.ANY)
    dma = pltpu.SemaphoreType.DMA
    gathers = 2 * CHUNKS * 4 * 4
    return pl.pallas_call(
        kernel,
        name="layer",
        out_shape=jax.ShapeDtypeStruct((T, T), BF16),
        in_specs=[vmem] * 7 + [hbm] + [vmem] * 3 + [hbm] * 6,
        out_specs=vmem,
        scratch_shapes=[
            pltpu.VMEM((HEAD, T), BF16),
            pltpu.VMEM((HEAD, T), BF16),
            pltpu.VMEM((1, T), jnp.int32),
            pltpu.VMEM((HEAD, D), BF16),
            pltpu.VMEM((D, 2 * T), BF16),
            pltpu.VMEM((D, T), BF16),
            pltpu.VMEM((D, 2 * T), BF16),
            pltpu.VMEM((T, D), BF16),
            pltpu.VMEM((N_TP, T, T), BF16),
            pltpu.VMEM((N_TP, T, T), BF16),
            pltpu.VMEM((8, T), F32),
            pltpu.VMEM((N_TP, 8, T), F32),
            pltpu.VMEM((N_TP, T, T), BF16),
            pltpu.VMEM((SLOTS, T), BF16),
            pltpu.VMEM((T, SLOTS), BF16),
            pltpu.VMEM((T, SLOTS), BF16),
            pltpu.VMEM((N_SP, CAP, T), BF16),
            pltpu.VMEM((SIDE, SIDE, N_SP, CAP, T), BF16),
            pltpu.VMEM((SIDE, SIDE, N_SP, CAP, T), BF16),
            pltpu.VMEM((N_SP, CAP, T), BF16),
            pltpu.VMEM((N_SP, CAP, T), BF16),
            pltpu.VMEM((N_TP, T, T), BF16),
            pltpu.VMEM((N_TP, T, T), BF16),
            pltpu.VMEM((T, T), F32),
            dma((7,)),
            dma((3,)),
            dma((3,)),
            dma((N_TP,)),
            dma((N_TP,)),
            dma((N_TP,)),
            dma((N_TP,)),
            dma((N_TP,)),
            dma((N_TP,)),
            dma((N_SP,)),
            dma((N_SP,)),
            dma((gathers,)),
            dma((gathers,)),
            dma((N_SP,)),
            dma((N_SP,)),
            dma((N_TP,)),
            dma((N_TP,)),
        ],
        compiler_params=pltpu.CompilerParams(collective_id=0, has_side_effects=True),
    )(
        stream,
        values_in,
        in_gate,
        out_gate,
        documents[None, :],
        conv_taps,
        head_gain[None, :],
        mix_weight,
        norm_gain[None, :],
        routes,
        route_weight,
        expert_gate,
        expert_up,
        expert_down,
        shared_gate,
        shared_up,
        shared_down,
    )


def solution(mesh):
    in_specs = (
        P("tp", "sp"),
        P("tp", "sp"),
        P("tp", "sp"),
        P("tp", "sp"),
        P("sp"),
        P(None, "tp"),
        P("tp"),
        P("tp", None),
        P("tp"),
        P("sp", None),
        P("sp", None),
        P("sp", None, "tp"),
        P("sp", None, "tp"),
        P("sp", None, "tp"),
        P(None, "tp"),
        P(None, "tp"),
        P("tp", None),
    )
    return jax.shard_map(
        local, mesh=mesh, in_specs=in_specs, out_specs=P("tp", "sp"), check_vma=False
    )
```

```python
import jax
import jax.numpy as jnp
from jax import lax
from jax.experimental import pallas as pl
from jax.experimental.pallas import tpu as pltpu
from jax.sharding import PartitionSpec as P

F32 = jnp.float32
BF16 = jnp.bfloat16
MESH = pl.DeviceIdType.MESH
EPS = 1e-06

D = 2048
T = 128
HEAD = 64
N_SP = 32
N_TP = 16
N_Z = 16
SIDE = 4
CAP = 24
TOP_K = 4
SLOTS = N_SP * CAP
DISTANCES = ((0, 1, -1, 2), (8, -7, 7, -6, 6, -5, 5, -4), (4, -3, 3, -2))
PLACES = [dz for chunk in DISTANCES for dz in chunk]
CHUNKS = len(DISTANCES)
SIZES = [2 * len(chunk) for chunk in DISTANCES]
STARTS = [sum(SIZES[:c]) for c in range(CHUNKS)]
STAGES = 9
GATHER = (4, 12, 8, 2)
EXPERT = (4, 4, 8, 4)
COPIES = sum(GATHER) + sum(EXPERT)
ALL = COPIES * CHUNKS + sum(GATHER)
LAG = 1.01
SHARED = {1: (0, 1), 2: (0, 2), 3: (0, 3), 4: (1, 3)}
SHARED_SEND_AFTER = (CHUNKS - 1, 7)


def dot(a, b, contract=((1,), (0,)), precision=None):
    return lax.dot_general(
        a, b, (contract, ((), ())), precision=precision, preferred_element_type=F32
    )


def iota(shape, dim):
    return lax.broadcasted_iota(jnp.int32, shape, dim)


def column_of(row, n):
    eye = iota((n, n), 0) == iota((n, n), 1)
    return jnp.sum(jnp.where(eye, jnp.broadcast_to(row, (n, n)), 0.0), axis=1, keepdims=True)


def kernel(
    stream,
    values_in,
    in_gate,
    out_gate,
    documents,
    conv_taps,
    head_gain,
    mix_weight,
    norm_gain,
    routes,
    route_weight,
    expert_gate,
    expert_up,
    expert_down,
    shared_gate,
    shared_up,
    shared_down,
    out,
    halo_v,
    halo_g,
    halo_d,
    mix_here,
    mix_w,
    w_gu,
    w_down,
    w_one,
    w_two,
    s_gu,
    s_down,
    head_all,
    gains,
    normed_all,
    pick,
    comb_hi,
    comb_lo,
    disp_out,
    rows_all,
    mid_all,
    part,
    direct,
    chain,
    chain_out,
    final,
    ret_out,
    ret_in,
    sh_part,
    sh_in,
    hidden,
    load_sem,
    down_s,
    down_r,
    halo_s,
    halo_r,
    mix_s,
    mix_r,
    swap_s,
    swap_r,
    head_s,
    head_r,
    gain_s,
    gain_r,
    nrm_s,
    nrm_r,
    disp_s,
    disp_r,
    gat_s,
    gat_r,
    ret_s,
    ret_r,
    sh_s,
    sh_r,
):
    sp = lax.axis_index("sp")
    tp = lax.axis_index("tp")
    z, core = sp // 2, sp % 2
    y, x = tp // SIDE, tp % SIDE

    def remote(src, dst, send, recv, **where):
        return pltpu.make_async_remote_copy(
            src_ref=src,
            dst_ref=dst,
            send_sem=send,
            recv_sem=recv,
            device_id=where,
            device_id_type=MESH,
        )

    barrier = pltpu.get_barrier_semaphore()

    @pl.loop(1, N_SP)
    def _(step):
        pl.semaphore_signal(
            barrier, inc=1, device_id={"sp": (sp + step) % N_SP}, device_id_type=MESH
        )

    @pl.loop(1, N_TP)
    def _(step):
        pl.semaphore_signal(
            barrier, inc=1, device_id={"tp": (tp + step) % N_TP}, device_id_type=MESH
        )

    loads = [
        pltpu.make_async_copy(src, dst, load_sem.at[i])
        for i, (src, dst) in enumerate(
            [
                (mix_weight, mix_here),
                (expert_down, w_down),
                (expert_down.at[y], w_one.at[y]),
                (expert_down.at[:, x], w_two.at[x]),
                (shared_gate, s_gu.at[:, pl.ds(0, T)]),
                (shared_up, s_gu.at[:, pl.ds(T, T)]),
                (shared_down, s_down),
                (expert_gate.at[0], w_gu.at[:, pl.ds(0, T)]),
                (expert_up.at[0], w_gu.at[:, pl.ds(T, T)]),
            ]
        )
    ]
    for load in loads:
        load.start()

    line = iota((T, T), 0)
    named = jnp.zeros((T, T), F32)
    weight = jnp.zeros((T, T), F32)
    for k in range(TOP_K):
        hit = routes[k : k + 1, :] == line
        named = jnp.where(hit, 1.0, named)
        weight = jnp.where(hit, route_weight[k : k + 1, :], weight)
    before = jnp.where(line < iota((T, T), 1), 1.0, 0.0).astype(BF16)
    earlier = dot(named.astype(BF16), before)
    slot = jnp.where(named > 0, earlier, 200.0)
    slot_t = slot.T.astype(BF16)
    slot = slot.astype(BF16)
    weight = weight.T

    def slot_number(shape, dim):
        number = iota(shape, dim).astype(F32)
        return number - CAP * jnp.floor((number + 0.5) * (1.0 / CAP))

    away = iota((SLOTS, T), 0) - CAP * iota((SLOTS, T), 1)
    owner = jnp.where((away >= 0) & (away < CAP), 1.0, 0.0).astype(BF16)
    taken = dot(owner, slot)
    pick[...] = jnp.where(taken == slot_number((SLOTS, T), 0), 1.0, 0.0).astype(BF16)
    away = iota((T, SLOTS), 1) - CAP * iota((T, SLOTS), 0)
    owner = jnp.where((away >= 0) & (away < CAP), 1.0, 0.0).astype(BF16)
    taken = dot(slot_t, owner) == slot_number((T, SLOTS), 1)
    weight_hi = weight.astype(BF16)
    weight_lo = (weight - weight_hi.astype(F32)).astype(BF16)
    comb_hi[...] = jnp.where(taken, dot(weight_hi, owner), 0.0).astype(BF16)
    comb_lo[...] = jnp.where(taken, dot(weight_lo, owner), 0.0).astype(BF16)

    pl.semaphore_wait(barrier, N_SP + N_TP - 2)

    behind = (sp + 1) % N_SP
    halos = [
        remote(src, dst, halo_s.at[i], halo_r.at[i], sp=behind)
        for i, (src, dst) in enumerate(
            [(values_in, halo_v), (in_gate, halo_g), (documents, halo_d)]
        )
    ]
    for halo in halos:
        halo.start()

    def to_plane(src_of, dst, send, recv):
        def copy(step):
            peer = (tp + step) % N_TP
            return remote(src_of(peer), dst, send.at[step], recv.at[step], tp=peer)

        return copy

    def start_plane(copy):
        @pl.loop(1, N_TP)
        def _(step):
            copy(step).start()

    def wait_plane(copy):
        @pl.loop(1, N_TP)
        def _(step):
            copy(step).wait_recv()

    rows = pl.ds(core * (HEAD // 2), HEAD // 2)

    def columns(peer):
        return mix_here.at[rows, pl.ds(pl.multiple_of(peer * T, T), T)]

    mix_copy = to_plane(columns, mix_w.at[core, tp], mix_s, mix_r)
    loads[0].wait()
    start_plane(mix_copy)
    mix_w[core, tp] = mix_here[rows, pl.ds(pl.multiple_of(tp * T, T), T)]
    gain_copy = to_plane(lambda peer: norm_gain, gains.at[tp], gain_s, gain_r)
    start_plane(gain_copy)
    gains[tp] = norm_gain[...]
    product = values_in[...].astype(F32) * in_gate[...].astype(F32)
    docs = jnp.broadcast_to(documents[...], (8, T))
    tap = [column_of(conv_taps[j : j + 1, :], HEAD) for j in range(3)]
    gain_col = column_of(head_gain[...], HEAD)
    for halo in halos:
        halo.wait_recv()
    product_before = halo_v[...].astype(F32) * halo_g[...].astype(F32)
    docs_before = jnp.where(sp == 0, -1, jnp.broadcast_to(halo_d[...], (8, T)))
    convolved = jnp.zeros((HEAD, T), F32)
    for j in range(3):
        back = 2 - j
        if back:
            shifted = jnp.where(
                iota((HEAD, T), 1) < back,
                pltpu.roll(product_before, back, 1),
                pltpu.roll(product, back, 1),
            )
            docs_then = jnp.where(
                iota((8, T), 1) < back,
                pltpu.roll(docs_before, back, 1),
                pltpu.roll(docs, back, 1),
            )
            same = jnp.where(docs_then == docs, 1.0, 0.0)[0:1, :]
            convolved = convolved + tap[j] * shifted * same
        else:
            convolved = convolved + tap[j] * product
    mixed = out_gate[...].astype(F32) * convolved
    spread = jnp.mean(mixed * mixed, axis=0, keepdims=True)
    heads = (mixed * lax.rsqrt(spread + EPS) * gain_col).T.astype(BF16)

    head_all[tp] = heads
    head_copy = to_plane(lambda peer: head_all.at[tp], head_all.at[tp], head_s, head_r)
    start_plane(head_copy)

    downs = []
    for n, way in enumerate((1, -1, 2)):
        to_y, to_x = (y + way + SIDE) % SIDE, (x + way + SIDE) % SIDE
        downs.append(
            remote(w_down.at[to_y], w_one.at[y], down_s.at[2 * n], down_r.at[2 * n], tp=SIDE * to_y + x)
        )
        downs.append(
            remote(
                w_down.at[:, to_x],
                w_two.at[x],
                down_s.at[2 * n + 1],
                down_r.at[2 * n + 1],
                tp=SIDE * y + to_x,
            )
        )
    for load in loads[1:4]:
        load.wait()
    for copy in downs:
        copy.start()
    wait_plane(mix_copy)
    swap = remote(mix_w.at[core], mix_w.at[core], swap_s, swap_r, sp=2 * z + 1 - core)
    swap.start()
    total = stream[...].astype(F32).T
    swap.wait_recv()
    wait_plane(head_copy)
    half = HEAD // 2
    all_heads = jnp.concatenate([head_all[j] for j in range(N_TP)], axis=1)
    all_mix = jnp.concatenate(
        [mix_w[c, j] for j in range(N_TP) for c in range(2)], axis=0
    )
    total = total + dot(all_heads, all_mix)
    hidden[...] = total
    normed = (total * norm_gain[...]).astype(BF16)

    normed_all[y, x] = normed
    disp_out[...] = dot(pick[...], normed).astype(BF16).reshape(N_SP, CAP, T)
    order = [(dz, other) for dz in PLACES for other in (0, 1)][1:]

    def disp_copy(dz, other):
        place = PLACES.index(dz)
        expert = 2 * ((z - dz + N_Z) % N_Z) + ((core + 1 + other) % 2 if dz else 1 - core)
        block = 2 * place + core
        return remote(
            disp_out.at[expert],
            rows_all.at[y, x, block],
            disp_s.at[2 * place + other],
            disp_r.at[block],
            sp=expert,
        )

    def arrived(dz, other):
        place = PLACES.index(dz)
        return 2 * place + (other if dz else 1 - core)

    for dz, other in order:
        disp_copy(dz, other).start()
    own = core
    rows_all[y, x, own] = disp_out[sp]

    def wait_disp(chunk):
        for dz, other in order:
            if dz in DISTANCES[chunk]:
                block = arrived(dz, other)
                remote(
                    disp_out.at[0], rows_all.at[y, x, block], disp_s.at[0], disp_r.at[block], sp=behind
                ).wait_recv()

    def at_x(way):
        return (x + way + SIDE) % SIDE

    def at_y(way):
        return (y + way + SIDE) % SIDE

    to_x = [SIDE * y + at_x(-1), SIDE * y + at_x(1)]
    to_y = [SIDE * at_y(-1) + x, SIDE * at_y(1) + x]
    ways = (-1, 1)

    def numbered(moves, base):
        return [
            remote(src, dst, gat_s.at[base + n], gat_r.at[base + n], tp=peer)
            for n, (src, dst, peer) in enumerate(moves)
        ]

    def gather_copies(buf, start, size, base, stage, parity):
        both = pl.ds(start, size)
        one, two = pl.ds(start, size // 2), pl.ds(start + size // 2, size // 2)
        if stage == 0:
            moves = [(buf.at[y, x, both], to[i]) for i in (0, 1) for to in (to_x, to_y)]
        elif stage == 1:
            moves = [
                (buf.at[y, at_x(-1), one], to_x[1]),
                (buf.at[at_y(-1), x, two], to_y[1]),
                (buf.at[y, at_x(1), two], to_x[0]),
                (buf.at[at_y(1), x, one], to_y[0]),
            ]
            for i in (0, 1):
                for way in ways:
                    moves += [(buf.at[y, at_x(way), one], to_y[i]), (buf.at[at_y(way), x, two], to_x[i])]
        elif stage == 2:
            moves = []
            for i in (0, 1):
                moves += [(buf.at[y, at_x(2), one], to_y[i]), (buf.at[at_y(2), x, two], to_x[i])]
            moves += [
                (buf.at[at_y(-1), at_x(1), one], to_y[1]),
                (buf.at[at_y(1), at_x(-1), two], to_x[1]),
                (buf.at[at_y(1), at_x(-1), one], to_y[0]),
                (buf.at[at_y(-1), at_x(1), two], to_x[0]),
            ]
        else:
            i = parity
            moves = [
                (buf.at[at_y(-ways[i]), at_x(2), one], to_y[i]),
                (buf.at[at_y(2), at_x(-ways[i]), two], to_x[i]),
            ]
        return numbered([(ref, ref, peer) for ref, peer in moves], base + sum(GATHER[:stage]))

    def row_copies(chunk, stage):
        return gather_copies(rows_all, STARTS[chunk], SIZES[chunk], COPIES * chunk, stage, chunk % 2)

    def normed_copies(stage):
        return gather_copies(normed_all, 0, T, COPIES * CHUNKS, stage, 1)

    def halves(chunk):
        size = SIZES[chunk] // 4
        quarter = [pl.ds(STARTS[chunk] + n * size, size) for n in range(4)]
        return quarter[:2], quarter[2:]

    def expert_copies(chunk, stage):
        size = SIZES[chunk] // 2
        one, two = pl.ds(STARTS[chunk], size), pl.ds(STARTS[chunk] + size, size)
        (one_a, one_b), (two_a, two_b) = halves(chunk)
        moves = []
        if stage == 0:
            for i in (0, 1):
                moves += [(mid_all.at[y, x, one], to_x[i]), (mid_all.at[y, x, two], to_y[i])]
            moves = [(ref, ref, peer) for ref, peer in moves]
        elif stage == 1:
            moves = [
                (mid_all.at[y, at_x(-1), one_a], to_x[1]),
                (mid_all.at[at_y(-1), x, two_a], to_y[1]),
                (mid_all.at[y, at_x(1), one_b], to_x[0]),
                (mid_all.at[at_y(1), x, two_b], to_y[0]),
            ]
            moves = [(ref, ref, peer) for ref, peer in moves]
        elif stage == 2:
            for at, to, (a, b) in ((at_y, to_y, (one_a, one_b)), (at_x, to_x, (two_a, two_b))):
                moves += [(part.at[at(2), a], chain.at[a], to[1]), (part.at[at(2), b], chain.at[b], to[0])]
            for at, to, (a, b) in ((at_y, to_y, (one_a, one_b)), (at_x, to_x, (two_a, two_b))):
                moves += [(part.at[at(1), b], direct.at[b], to[1]), (part.at[at(-1), a], direct.at[a], to[0])]
        else:
            for to, (a, b) in ((to_y, (one_a, one_b)), (to_x, (two_a, two_b))):
                moves += [(chain_out.at[a], final.at[a], to[1]), (chain_out.at[b], final.at[b], to[0])]
        return numbered(moves, COPIES * chunk + sum(GATHER) + sum(EXPERT[:stage]))

    def go(copies):
        for copy in copies:
            copy.start()

    def got(copies):
        for copy in copies:
            copy.wait_recv()

    def rows_of(ref):
        return ref.reshape(ref.shape[0] * CAP, T)

    def silu(v):
        return v / (1.0 + jnp.exp(-v))

    def gated(blocks, weights):
        squares = jnp.zeros(blocks[0].shape, F32)
        for j, block in enumerate(blocks):
            wide = block.astype(F32)
            squares = squares + wide * wide * (1.0 / (gains[j] * gains[j]))
        scale = lax.rsqrt(jnp.sum(squares, axis=1, keepdims=True) / D + EPS)
        pair = dot(jnp.concatenate(blocks, axis=1), weights) * scale
        return (silu(pair[:, :T]) * pair[:, T:]).astype(BF16)

    def gate_up(chunk):
        here = pl.ds(STARTS[chunk], SIZES[chunk])
        blocks = [rows_of(rows_all[i, j, here]) for i in range(SIDE) for j in range(SIDE)]
        mid = gated(blocks, w_gu[...])
        mid_all[y, x, here] = mid.reshape(SIZES[chunk], CAP, T)

    def down(chunk):
        size = SIZES[chunk] // 2
        for half in range(2):
            here = pl.ds(STARTS[chunk] + size * half, size)
            line = [mid_all[y, k, here] if half == 0 else mid_all[k, x, here] for k in range(SIDE)]
            line = jnp.concatenate([rows_of(block) for block in line], axis=1)
            weights = w_two if half else w_one
            for q in range(0, SIDE, 2):
                pair = jnp.concatenate(
                    [weights[q + n].reshape(SIDE * T, T) for n in range(2)], axis=1
                )
                result = dot(line, pair).astype(BF16)
                for n in range(2):
                    part[q + n, here] = result[:, n * T : (n + 1) * T].reshape(size, CAP, T)

    def relay(chunk):
        for at, (a, b) in zip((at_y, at_x), halves(chunk)):
            for rows, q in ((a, at(1)), (b, at(-1))):
                chain_out[rows] = (chain[rows].astype(F32) + part[q, rows].astype(F32)).astype(BF16)

    def finish(chunk):
        for own_place, (a, b) in zip((y, x), halves(chunk)):
            for rows in (a, b):
                value = part[own_place, rows].astype(F32) + direct[rows].astype(F32)
                ret_out[rows] = (value + final[rows].astype(F32)).astype(BF16)

    def ret_copy(dz, other):
        place = PLACES.index(dz)
        group_core = (core + 1 + other) % 2 if dz else 1 - core
        group = 2 * ((z + dz + N_Z) % N_Z) + group_core
        return remote(
            ret_out.at[2 * place + group_core],
            ret_in.at[sp],
            ret_s.at[2 * place + other],
            ret_r.at[2 * place + core],
            sp=group,
        )

    def start_ret(chunk):
        for dz, other in order:
            if dz in DISTANCES[chunk]:
                ret_copy(dz, other).start()

    def shared_expert():
        for load in loads[4:7]:
            load.wait()
        mid = gated([normed_all[i, j] for i in range(SIDE) for j in range(SIDE)], s_gu[...])
        for j in range(N_TP // 2):
            part = dot(mid, s_down[:, 2 * T * j : 2 * T * (j + 1)]).astype(BF16)
            sh_part[2 * j] = part[:, :T]
            sh_part[2 * j + 1] = part[:, T:]

    sh_copy = to_plane(lambda peer: sh_part.at[peer], sh_in.at[tp], sh_s, sh_r)

    def advance(chunk, stage):
        if stage == 0:
            wait_disp(chunk)
            go(row_copies(chunk, 0))
        elif stage < 4:
            got(row_copies(chunk, stage - 1))
            go(row_copies(chunk, stage))
        elif stage == 4:
            got(row_copies(chunk, 3))
            gate_up(chunk)
            go(expert_copies(chunk, 0))
        elif stage == 5:
            got(expert_copies(chunk, 0))
            go(expert_copies(chunk, 1))
        elif stage == 6:
            got(expert_copies(chunk, 1))
            down(chunk)
            go(expert_copies(chunk, 2))
        elif stage == 7:
            got(expert_copies(chunk, 2))
            relay(chunk)
            go(expert_copies(chunk, 3))
        else:
            got(expert_copies(chunk, 3))
            finish(chunk)
            start_ret(chunk)

    go(normed_copies(0))
    steps = sorted((stage + LAG * chunk, chunk, stage) for chunk in range(CHUNKS) for stage in range(STAGES))
    for _, chunk, stage in steps:
        if (chunk, stage) == (0, 4):
            wait_plane(gain_copy)
            for load in loads[7:]:
                load.wait()
            got(downs)
        advance(chunk, stage)
        for turn, after in SHARED.items():
            if after == (chunk, stage):
                got(normed_copies(turn - 1))
                if turn < 4:
                    go(normed_copies(turn))
                else:
                    shared_expert()
                    sh_in[tp] = sh_part[tp]
        if (chunk, stage) == SHARED_SEND_AFTER:
            start_plane(sh_copy)
        if (chunk, stage) == (0, 8):
            ret_in[sp] = ret_out[own]

    wait_plane(sh_copy)
    total = hidden[...]
    for j in range(N_TP):
        total = total + sh_in[j].astype(F32)

    for halo in halos:
        halo.wait_send()
    swap.wait_send()
    for copy in (mix_copy, gain_copy, head_copy, sh_copy):

        @pl.loop(1, N_TP)
        def _(step, copy=copy):
            copy(step).wait_send()

    for dz, other in order:
        disp_copy(dz, other).wait_send()
    sent = downs[:]
    for stage in range(4):
        sent += normed_copies(stage)
        for chunk in range(CHUNKS):
            sent += row_copies(chunk, stage) + expert_copies(chunk, stage)
    for copy in sent:
        copy.wait_send()

    for dz, other in order:
        block = arrived(dz, other)
        remote(ret_out.at[0], ret_in.at[0], ret_s.at[0], ret_r.at[block], sp=behind).wait_recv()
    returned = ret_in[...].reshape(SLOTS, T)
    total = total + dot(comb_hi[...], returned) + dot(comb_lo[...], returned)
    out[...] = total.T.astype(BF16)
    for dz, other in order:
        ret_copy(dz, other).wait_send()


def local(
    stream,
    values_in,
    in_gate,
    out_gate,
    documents,
    conv_taps,
    head_gain,
    mix_weight,
    norm_gain,
    routes,
    route_weight,
    expert_gate,
    expert_up,
    expert_down,
    shared_gate,
    shared_up,
    shared_down,
):
    vmem = pl.BlockSpec(memory_space=pltpu.VMEM)
    hbm = pl.BlockSpec(memory_space=pl.ANY)
    dma = pltpu.SemaphoreType.DMA
    return pl.pallas_call(
        kernel,
        name="layer",
        out_shape=jax.ShapeDtypeStruct((T, T), BF16),
        in_specs=[vmem] * 7 + [hbm] + [vmem] * 3 + [hbm] * 6,
        out_specs=vmem,
        scratch_shapes=[
            pltpu.VMEM((HEAD, T), BF16),
            pltpu.VMEM((HEAD, T), BF16),
            pltpu.VMEM((1, T), jnp.int32),
            pltpu.VMEM((HEAD, D), BF16),
            pltpu.VMEM((2, N_TP, HEAD // 2, T), BF16),
            pltpu.VMEM((D, 2 * T), BF16),
            pltpu.VMEM((SIDE, SIDE, T, T), BF16),
            pltpu.VMEM((SIDE, SIDE, T, T), BF16),
            pltpu.VMEM((SIDE, SIDE, T, T), BF16),
            pltpu.VMEM((D, 2 * T), BF16),
            pltpu.VMEM((T, D), BF16),
            pltpu.VMEM((N_TP, T, HEAD), BF16),
            pltpu.VMEM((N_TP, 1, T), F32),
            pltpu.VMEM((SIDE, SIDE, T, T), BF16),
            pltpu.VMEM((SLOTS, T), BF16),
            pltpu.VMEM((T, SLOTS), BF16),
            pltpu.VMEM((T, SLOTS), BF16),
            pltpu.VMEM((N_SP, CAP, T), BF16),
            pltpu.VMEM((SIDE, SIDE, N_SP, CAP, T), BF16),
            pltpu.VMEM((SIDE, SIDE, N_SP, CAP, T), BF16),
            pltpu.VMEM((SIDE, N_SP, CAP, T), BF16),
            pltpu.VMEM((N_SP, CAP, T), BF16),
            pltpu.VMEM((N_SP, CAP, T), BF16),
            pltpu.VMEM((N_SP, CAP, T), BF16),
            pltpu.VMEM((N_SP, CAP, T), BF16),
            pltpu.VMEM((N_SP, CAP, T), BF16),
            pltpu.VMEM((N_SP, CAP, T), BF16),
            pltpu.VMEM((N_TP, T, T), BF16),
            pltpu.VMEM((N_TP, T, T), BF16),
            pltpu.VMEM((T, T), F32),
            dma((9,)),
            dma((6,)),
            dma((6,)),
            dma((3,)),
            dma((3,)),
            dma((N_TP,)),
            dma((N_TP,)),
            dma,
            dma,
            dma((N_TP,)),
            dma((N_TP,)),
            dma((N_TP,)),
            dma((N_TP,)),
            dma((N_TP,)),
            dma((N_TP,)),
            dma((N_SP,)),
            dma((N_SP,)),
            dma((ALL,)),
            dma((ALL,)),
            dma((N_SP,)),
            dma((N_SP,)),
            dma((N_TP,)),
            dma((N_TP,)),
        ],
        compiler_params=pltpu.CompilerParams(collective_id=0, has_side_effects=True),
    )(
        stream,
        values_in,
        in_gate,
        out_gate,
        documents[None, :],
        conv_taps,
        head_gain[None, :],
        mix_weight,
        norm_gain[None, :],
        routes.T,
        route_weight.T,
        expert_gate,
        expert_up,
        expert_down.reshape(SIDE, SIDE, T, T),
        shared_gate,
        shared_up,
        shared_down,
    )


def solution(mesh):
    in_specs = (
        P("tp", "sp"),
        P("tp", "sp"),
        P("tp", "sp"),
        P("tp", "sp"),
        P("sp"),
        P(None, "tp"),
        P("tp"),
        P("tp", None),
        P("tp"),
        P("sp", None),
        P("sp", None),
        P("sp", None, "tp"),
        P("sp", None, "tp"),
        P("sp", None, "tp"),
        P(None, "tp"),
        P(None, "tp"),
        P("tp", None),
    )
    return jax.shard_map(
        local, mesh=mesh, in_specs=in_specs, out_specs=P("tp", "sp"), check_vma=False
    )
```

```python
import jax
import jax.numpy as jnp
from jax import lax
from jax.experimental import pallas as pl
from jax.experimental.pallas import tpu as pltpu
from jax.sharding import PartitionSpec as P

F32 = jnp.float32
BF16 = jnp.bfloat16
MESH = pl.DeviceIdType.MESH
EPS = 1e-06

D = 2048
T = 128
HEAD = 64
N_SP = 32
N_TP = 16
N_Z = 16
SIDE = 4
CAP = 24
TOP_K = 4
SLOTS = N_SP * CAP
DISTANCES = ((0, 1, -1, 2), (8, -7, 7, -6, 6, -5, 5, -4), (4, -3, 3, -2))
PLACES = [dz for chunk in DISTANCES for dz in chunk]
CHUNKS = len(DISTANCES)
SIZES = [2 * len(chunk) for chunk in DISTANCES]
STARTS = [sum(SIZES[:c]) for c in range(CHUNKS)]
DIRECT = (True, False, True)
STEPS = 5
LAG = 1.01
SHARED = ((1, 0), (1, 1), (1, 3))
SHARED_SEND_AFTER = (CHUNKS - 1, -2)


def dot(a, b, contract=((1,), (0,)), precision=None):
    return lax.dot_general(
        a, b, (contract, ((), ())), precision=precision, preferred_element_type=F32
    )


def iota(shape, dim):
    return lax.broadcasted_iota(jnp.int32, shape, dim)


def column_of(row, n):
    eye = iota((n, n), 0) == iota((n, n), 1)
    return jnp.sum(jnp.where(eye, jnp.broadcast_to(row, (n, n)), 0.0), axis=1, keepdims=True)


def kernel(
    stream,
    values_in,
    in_gate,
    out_gate,
    documents,
    conv_taps,
    head_gain,
    mix_weight,
    norm_gain,
    routes,
    route_weight,
    expert_gate,
    expert_up,
    expert_down,
    shared_gate,
    shared_up,
    shared_down,
    out,
    halo_v,
    halo_g,
    halo_d,
    mix_here,
    mix_w,
    w_gu,
    w_down,
    w_one,
    w_two,
    s_gu,
    s_down,
    head_all,
    gains,
    normed_all,
    pick,
    comb_hi,
    comb_lo,
    disp_out,
    rows_all,
    mid_all,
    part,
    direct,
    ret_out,
    ret_in,
    sh_part,
    sh_in,
    hidden,
    load_sem,
    down_s,
    down_r,
    halo_s,
    halo_r,
    mix_s,
    mix_r,
    swap_s,
    swap_r,
    head_s,
    head_r,
    tail_s,
    tail_r,
    gain_s,
    gain_r,
    disp_s,
    disp_r,
    gat_s,
    gat_r,
    ret_s,
    ret_r,
    sh_s,
    sh_r,
):
    sp = lax.axis_index("sp")
    tp = lax.axis_index("tp")
    z, core = sp // 2, sp % 2
    y, x = tp // SIDE, tp % SIDE

    def remote(src, dst, send, recv, **where):
        return pltpu.make_async_remote_copy(
            src_ref=src,
            dst_ref=dst,
            send_sem=send,
            recv_sem=recv,
            device_id=where,
            device_id_type=MESH,
        )

    barrier = pltpu.get_barrier_semaphore()

    @pl.loop(1, N_SP)
    def _(step):
        pl.semaphore_signal(
            barrier, inc=1, device_id={"sp": (sp + step) % N_SP}, device_id_type=MESH
        )

    @pl.loop(1, N_TP)
    def _(step):
        pl.semaphore_signal(
            barrier, inc=1, device_id={"tp": (tp + step) % N_TP}, device_id_type=MESH
        )

    loads = [
        pltpu.make_async_copy(src, dst, load_sem.at[i])
        for i, (src, dst) in enumerate(
            [
                (mix_weight, mix_here),
                (expert_down, w_down),
                (expert_down.at[y], w_one.at[y]),
                (expert_down.at[:, x], w_two.at[x]),
                (shared_gate, s_gu.at[:, pl.ds(0, T)]),
                (shared_up, s_gu.at[:, pl.ds(T, T)]),
                (shared_down, s_down),
                (expert_gate.at[0], w_gu.at[:, pl.ds(0, T)]),
                (expert_up.at[0], w_gu.at[:, pl.ds(T, T)]),
            ]
        )
    ]
    for load in loads:
        load.start()

    line = iota((T, T), 0)
    named = jnp.zeros((T, T), F32)
    weight = jnp.zeros((T, T), F32)
    for k in range(TOP_K):
        hit = routes[k : k + 1, :] == line
        named = jnp.where(hit, 1.0, named)
        weight = jnp.where(hit, route_weight[k : k + 1, :], weight)
    before = jnp.where(line < iota((T, T), 1), 1.0, 0.0).astype(BF16)
    earlier = dot(named.astype(BF16), before)
    slot = jnp.where(named > 0, earlier, 200.0)
    slot_t = slot.T.astype(BF16)
    slot = slot.astype(BF16)
    weight = weight.T

    def slot_number(shape, dim):
        number = iota(shape, dim).astype(F32)
        return number - CAP * jnp.floor((number + 0.5) * (1.0 / CAP))

    away = iota((SLOTS, T), 0) - CAP * iota((SLOTS, T), 1)
    owner = jnp.where((away >= 0) & (away < CAP), 1.0, 0.0).astype(BF16)
    taken = dot(owner, slot)
    pick[...] = jnp.where(taken == slot_number((SLOTS, T), 0), 1.0, 0.0).astype(BF16)
    away = iota((T, SLOTS), 1) - CAP * iota((T, SLOTS), 0)
    owner = jnp.where((away >= 0) & (away < CAP), 1.0, 0.0).astype(BF16)
    taken = dot(slot_t, owner) == slot_number((T, SLOTS), 1)
    weight_hi = weight.astype(BF16)
    weight_lo = (weight - weight_hi.astype(F32)).astype(BF16)
    comb_hi[...] = jnp.where(taken, dot(weight_hi, owner), 0.0).astype(BF16)
    comb_lo[...] = jnp.where(taken, dot(weight_lo, owner), 0.0).astype(BF16)

    pl.semaphore_wait(barrier, N_SP + N_TP - 2)

    behind = (sp + 1) % N_SP
    halos = [
        remote(src, dst, halo_s.at[i], halo_r.at[i], sp=behind)
        for i, (src, dst) in enumerate(
            [(values_in, halo_v), (in_gate, halo_g), (documents, halo_d)]
        )
    ]
    for halo in halos:
        halo.start()

    def arrive(ref, recv):
        remote(ref, ref, recv, recv, sp=behind).wait_recv()

    def leave(ref, send):
        remote(ref, ref, send, send, sp=behind).wait_send()

    def to_plane(src_of, dst, send, recv):
        @pl.loop(1, N_TP)
        def _(step):
            peer = (tp + step) % N_TP
            remote(src_of(peer), dst, send, recv, tp=peer).start()

    rows = pl.ds(pl.multiple_of(core * (HEAD // 2), HEAD // 2), HEAD // 2)

    def columns(peer):
        return mix_here.at[rows, pl.ds(pl.multiple_of(peer * T, T), T)]

    loads[0].wait()
    to_plane(columns, mix_w.at[tp, rows], mix_s, mix_r)
    mix_w[tp, rows] = mix_here[rows, pl.ds(pl.multiple_of(tp * T, T), T)]

    product = values_in[...].astype(F32) * in_gate[...].astype(F32)
    docs = jnp.broadcast_to(documents[...], (8, T))
    tap = [column_of(conv_taps[j : j + 1, :], HEAD) for j in range(3)]
    gain_col = column_of(head_gain[...], HEAD)

    def heads_after(product_before, docs_before):
        convolved = jnp.zeros((HEAD, T), F32)
        for j in range(3):
            back = 2 - j
            if back:
                shifted = jnp.where(
                    iota((HEAD, T), 1) < back,
                    pltpu.roll(product_before, back, 1),
                    pltpu.roll(product, back, 1),
                )
                docs_then = jnp.where(
                    iota((8, T), 1) < back,
                    pltpu.roll(docs_before, back, 1),
                    pltpu.roll(docs, back, 1),
                )
                same = jnp.where(docs_then == docs, 1.0, 0.0)[0:1, :]
                convolved = convolved + tap[j] * shifted * same
            else:
                convolved = convolved + tap[j] * product
        mixed = out_gate[...].astype(F32) * convolved
        spread = jnp.mean(mixed * mixed, axis=0, keepdims=True)
        heads = (mixed * lax.rsqrt(spread + EPS) * gain_col).T
        return jnp.concatenate([heads[:HEAD], heads[HEAD:]], axis=1).astype(BF16)

    first, rest = pl.ds(0, 8), pl.ds(8, HEAD - 8)
    head_all[tp, rest] = heads_after(product, docs)[8:]
    to_plane(lambda peer: head_all.at[tp, rest], head_all.at[tp, rest], head_s, head_r)
    for halo in halos:
        halo.wait_recv()
    product_before = halo_v[...].astype(F32) * halo_g[...].astype(F32)
    docs_before = jnp.where(sp == 0, -1, jnp.broadcast_to(halo_d[...], (8, T)))
    head_all[tp, first] = heads_after(product_before, docs_before)[:8]
    to_plane(lambda peer: head_all.at[tp, first], head_all.at[tp, first], tail_s, tail_r)

    others = pl.ds(0, N_TP - 1)
    arrive(mix_w.at[others, pl.ds(0, HEAD // 2)], mix_r)
    swap = remote(mix_w.at[:, rows], mix_w.at[:, rows], swap_s, swap_r, sp=2 * z + 1 - core)
    swap.start()
    for load in loads[1:4]:
        load.wait()
    for way in (2, -1, 1):
        beside_y, beside_x = (y + way + SIDE) % SIDE, (x + way + SIDE) % SIDE
        remote(
            w_down.at[beside_y], w_one.at[y], down_s.at[0], down_r.at[0], tp=SIDE * beside_y + x
        ).start()
        remote(
            w_down.at[:, beside_x], w_two.at[x], down_s.at[1], down_r.at[1], tp=SIDE * y + beside_x
        ).start()

    total = stream[...].astype(F32).T
    swap.wait_recv()
    arrive(head_all.at[others, rest], head_r)
    arrive(head_all.at[others, first], tail_r)
    all_heads = jnp.concatenate([head_all[j] for j in range(N_TP)], axis=1)
    none = jnp.zeros((HEAD, T), BF16)
    early = jnp.concatenate([v for j in range(N_TP) for v in (mix_w[j], none)], axis=0)
    late = jnp.concatenate([v for j in range(N_TP) for v in (none, mix_w[j])], axis=0)
    mixer = dot(all_heads, jnp.concatenate([early, late], axis=1))
    total = total + jnp.concatenate([mixer[:, :T], mixer[:, T:]], axis=0)
    hidden[...] = total
    normed = (total * norm_gain[...]).astype(BF16)

    normed_all[y, x] = normed
    disp_out[...] = dot(pick[...], normed).astype(BF16).reshape(N_SP, CAP, T)
    order = [(dz, other) for dz in PLACES for other in (0, 1)][1:]

    def disp_copy(dz, other):
        place = PLACES.index(dz)
        expert = 2 * ((z - dz + N_Z) % N_Z) + ((core + 1 + other) % 2 if dz else 1 - core)
        block = 2 * place + core
        return remote(
            disp_out.at[expert],
            rows_all.at[y, x, block],
            disp_s,
            disp_r.at[next(c for c in range(CHUNKS) if dz in DISTANCES[c])],
            sp=expert,
        )

    for dz, other in order:
        disp_copy(dz, other).start()
    own = core
    rows_all[y, x, own] = disp_out[sp]

    def wait_disp(chunk):
        count = SIZES[chunk] - (chunk == 0)
        arrive(rows_all.at[y, x, pl.ds(STARTS[chunk], count)], disp_r.at[chunk])

    def at_x(way):
        return (x + way + SIDE) % SIDE

    def at_y(way):
        return (y + way + SIDE) % SIDE

    to_x = [SIDE * y + at_x(-1), SIDE * y + at_x(1)]
    to_y = [SIDE * at_y(-1) + x, SIDE * at_y(1) + x]
    ways = (-1, 1)

    def numbered(moves, index):
        return [
            remote(src, dst, gat_s.at[index], gat_r.at[index], tp=peer) for src, dst, peer in moves
        ]

    to_x.append(SIDE * y + at_x(2))
    to_y.append(SIDE * at_y(2) + x)

    def gather_copies(buf, start, size, index, stage, short):
        both = pl.ds(start, size)
        one, two = pl.ds(start, size // 2), pl.ds(start + size // 2, size // 2)
        a, b = pl.ds(start, size // 4), pl.ds(start + size // 4, size // 4)
        c, d = pl.ds(start + size // 2, size // 4), pl.ds(start + size // 2 + size // 4, size // 4)
        if stage == 0:
            moves = [(buf.at[y, x, both], to[i]) for i in (2, 0, 1) for to in (to_x, to_y)]
        elif stage == 1:
            moves = []
            for way in (-1, 1, 2):
                for i in (2, 0, 1) if short else (0, 1):
                    moves += [(buf.at[y, at_x(way), one], to_y[i]), (buf.at[at_y(way), x, two], to_x[i])]
        else:
            moves = [
                (buf.at[at_y(-1), at_x(1), one], to_y[1]),
                (buf.at[at_y(1), at_x(-1), two], to_x[1]),
                (buf.at[at_y(1), at_x(-1), one], to_y[0]),
                (buf.at[at_y(-1), at_x(1), two], to_x[0]),
                (buf.at[at_y(-1), at_x(2), a], to_y[1]),
                (buf.at[at_y(2), at_x(-1), c], to_x[1]),
                (buf.at[at_y(1), at_x(2), b], to_y[0]),
                (buf.at[at_y(2), at_x(1), d], to_x[0]),
            ]
        return numbered([(ref, ref, peer) for ref, peer in moves], index)

    def thirds(stage, short):
        return (2, 3 if short else 2, 1)[stage]

    def row_copies(chunk, stage):
        index = STEPS * chunk + stage
        start, size, short = STARTS[chunk], SIZES[chunk], DIRECT[chunk]
        copies = lambda: gather_copies(rows_all, start, size, index, stage, short)
        count = thirds(stage, DIRECT[chunk])
        return copies, rows_all.at[pl.ds(0, count), pl.ds(0, 3), pl.ds(0, SIZES[chunk])], index

    def normed_copies(stage):
        index = STEPS * CHUNKS + stage
        copies = lambda: gather_copies(normed_all, 0, T, index, stage, False)
        return copies, normed_all.at[pl.ds(0, thirds(stage, False)), pl.ds(0, 3)], index

    def expert_copies(chunk, stage):
        size = SIZES[chunk] // 2
        one, two = pl.ds(STARTS[chunk], size), pl.ds(STARTS[chunk] + size, size)
        moves = []
        for i, way in ((2, 2), (0, -1), (1, 1)):
            if stage == 0:
                moves.append((mid_all.at[y, x, one], mid_all.at[y, x, one], to_x[i]))
                moves.append((mid_all.at[y, x, two], mid_all.at[y, x, two], to_y[i]))
            else:
                moves.append((part.at[at_y(way), one], direct.at[i, one], to_y[i]))
                moves.append((part.at[at_x(way), two], direct.at[i, two], to_x[i]))
        index = STEPS * chunk + 3 + stage
        return lambda: numbered(moves, index), direct.at[:, pl.ds(0, SIZES[chunk])], index

    def go(kind):
        for copy in kind[0]():
            copy.start()

    def got(kind):
        arrive(kind[1], gat_r.at[kind[2]])

    def rows_of(ref):
        return ref.reshape(ref.shape[0] * CAP, T)

    def silu(v):
        return v / (1.0 + jnp.exp(-v))

    def gated(blocks, weights):
        squares = jnp.zeros(blocks[0].shape, F32)
        for j, block in enumerate(blocks):
            wide = block.astype(F32)
            squares = squares + wide * wide * (1.0 / (gains[j] * gains[j]))
        scale = lax.rsqrt(jnp.sum(squares, axis=1, keepdims=True) / D + EPS)
        pair = dot(jnp.concatenate(blocks, axis=1), weights) * scale
        return (silu(pair[:, :T]) * pair[:, T:]).astype(BF16)

    def gate_up(chunk):
        here = pl.ds(STARTS[chunk], SIZES[chunk])
        blocks = [rows_of(rows_all[i, j, here]) for i in range(SIDE) for j in range(SIDE)]
        mid = gated(blocks, w_gu[...])
        mid_all[y, x, here] = mid.reshape(SIZES[chunk], CAP, T)

    def down(chunk):
        size = SIZES[chunk] // 2
        for half in range(2):
            here = pl.ds(STARTS[chunk] + size * half, size)
            line = [mid_all[y, k, here] if half == 0 else mid_all[k, x, here] for k in range(SIDE)]
            line = jnp.concatenate([rows_of(block) for block in line], axis=1)
            weights = w_two if half else w_one
            for q in range(0, SIDE, 2):
                pair = jnp.concatenate(
                    [weights[q + n].reshape(SIDE * T, T) for n in range(2)], axis=1
                )
                result = dot(line, pair).astype(BF16)
                for n in range(2):
                    part[q + n, here] = result[:, n * T : (n + 1) * T].reshape(size, CAP, T)

    def finish(chunk):
        size = SIZES[chunk] // 2
        for half in range(2):
            here = pl.ds(STARTS[chunk] + size * half, size)
            value = part[x if half else y, here].astype(F32)
            for i in range(3):
                value = value + direct[i, here].astype(F32)
            ret_out[here] = value.astype(BF16)

    def ret_copy(dz, other):
        place = PLACES.index(dz)
        group_core = (core + 1 + other) % 2 if dz else 1 - core
        group = 2 * ((z + dz + N_Z) % N_Z) + group_core
        return remote(
            ret_out.at[2 * place + group_core],
            ret_in.at[sp],
            ret_s,
            ret_r,
            sp=group,
        )

    def start_ret(chunk):
        for dz, other in order:
            if dz in DISTANCES[chunk]:
                ret_copy(dz, other).start()

    def shared_expert():
        for load in loads[4:7]:
            load.wait()
        mid = gated([normed_all[i, j] for i in range(SIDE) for j in range(SIDE)], s_gu[...])
        for j in range(N_TP // 2):
            part = dot(mid, s_down[:, 2 * T * j : 2 * T * (j + 1)]).astype(BF16)
            sh_part[2 * j] = part[:, :T]
            sh_part[2 * j + 1] = part[:, T:]

    def row_stages(chunk):
        return 2 if DIRECT[chunk] else 3

    def advance(chunk, stage):
        rows = row_stages(chunk)
        if stage == 0:
            wait_disp(chunk)
            go(row_copies(chunk, 0))
        elif stage < rows:
            got(row_copies(chunk, stage - 1))
            go(row_copies(chunk, stage))
        elif stage == rows:
            got(row_copies(chunk, rows - 1))
            gate_up(chunk)
            go(expert_copies(chunk, 0))
        elif stage == rows + 1:
            got(expert_copies(chunk, 0))
            down(chunk)
            go(expert_copies(chunk, 1))
        else:
            got(expert_copies(chunk, 1))
            finish(chunk)
            start_ret(chunk)

    go(normed_copies(0))
    to_plane(lambda peer: norm_gain, gains.at[tp], gain_s, gain_r)
    gains[tp] = norm_gain[...]
    steps = sorted(
        (stage + LAG * chunk, chunk, stage)
        for chunk in range(CHUNKS)
        for stage in range(row_stages(chunk) + 3)
    )
    for _, chunk, stage in steps:
        left = stage - row_stages(chunk) - 3
        if (chunk, left) == (0, -3):
            arrive(gains.at[others], gain_r)
            for load in loads[7:]:
                load.wait()
        if (chunk, left) == (0, -2):
            arrive(w_one.at[pl.ds(0, 3)], down_r.at[0])
            arrive(w_two.at[pl.ds(0, 3)], down_r.at[1])
        advance(chunk, stage)
        for turn, after in enumerate(SHARED):
            if after == (chunk, stage):
                got(normed_copies(turn))
                if turn < 2:
                    go(normed_copies(turn + 1))
                else:
                    shared_expert()
                    sh_in[tp] = sh_part[tp]
        if (chunk, left) == SHARED_SEND_AFTER:
            to_plane(lambda peer: sh_part.at[peer], sh_in.at[tp], sh_s, sh_r)
        if (chunk, left) == (0, -1):
            ret_in[sp] = ret_out[own]

    arrive(sh_in.at[others], sh_r)
    total = hidden[...]
    for j in range(N_TP):
        total = total + sh_in[j].astype(F32)

    for halo in halos:
        halo.wait_send()
    swap.wait_send()
    for ref, send in (
        (mix_w.at[others, pl.ds(0, HEAD // 2)], mix_s),
        (head_all.at[others, rest], head_s),
        (head_all.at[others, first], tail_s),
        (gains.at[others], gain_s),
        (w_one.at[pl.ds(0, 3)], down_s.at[0]),
        (w_two.at[pl.ds(0, 3)], down_s.at[1]),
        (disp_out.at[pl.ds(0, N_SP - 1)], disp_s),
        (sh_in.at[others], sh_s),
    ):
        leave(ref, send)
    kinds = [normed_copies(stage) for stage in range(3)]
    for chunk in range(CHUNKS):
        kinds += [row_copies(chunk, stage) for stage in range(row_stages(chunk))]
        kinds += [expert_copies(chunk, stage) for stage in range(2)]
    for _, ref, index in kinds:
        leave(ref, gat_s.at[index])

    arrive(ret_in.at[pl.ds(0, N_SP - 1)], ret_r)
    returned = ret_in[...].reshape(SLOTS, T)
    total = total + dot(comb_hi[...], returned) + dot(comb_lo[...], returned)
    out[...] = total.T.astype(BF16)
    leave(ret_in.at[pl.ds(0, N_SP - 1)], ret_s)


def local(
    stream,
    values_in,
    in_gate,
    out_gate,
    documents,
    conv_taps,
    head_gain,
    mix_weight,
    norm_gain,
    routes,
    route_weight,
    expert_gate,
    expert_up,
    expert_down,
    shared_gate,
    shared_up,
    shared_down,
):
    vmem = pl.BlockSpec(memory_space=pltpu.VMEM)
    hbm = pl.BlockSpec(memory_space=pl.ANY)
    dma = pltpu.SemaphoreType.DMA
    return pl.pallas_call(
        kernel,
        name="layer",
        out_shape=jax.ShapeDtypeStruct((T, T), BF16),
        in_specs=[vmem] * 7 + [hbm] + [vmem] * 3 + [hbm] * 6,
        out_specs=vmem,
        scratch_shapes=[
            pltpu.VMEM((HEAD, T), BF16),
            pltpu.VMEM((HEAD, T), BF16),
            pltpu.VMEM((1, T), jnp.int32),
            pltpu.VMEM((HEAD, D), BF16),
            pltpu.VMEM((N_TP, HEAD, T), BF16),
            pltpu.VMEM((D, 2 * T), BF16),
            pltpu.VMEM((SIDE, SIDE, T, T), BF16),
            pltpu.VMEM((SIDE, SIDE, T, T), BF16),
            pltpu.VMEM((SIDE, SIDE, T, T), BF16),
            pltpu.VMEM((D, 2 * T), BF16),
            pltpu.VMEM((T, D), BF16),
            pltpu.VMEM((N_TP, HEAD, T), BF16),
            pltpu.VMEM((N_TP, 1, T), F32),
            pltpu.VMEM((SIDE, SIDE, T, T), BF16),
            pltpu.VMEM((SLOTS, T), BF16),
            pltpu.VMEM((T, SLOTS), BF16),
            pltpu.VMEM((T, SLOTS), BF16),
            pltpu.VMEM((N_SP, CAP, T), BF16),
            pltpu.VMEM((SIDE, SIDE, N_SP, CAP, T), BF16),
            pltpu.VMEM((SIDE, SIDE, N_SP, CAP, T), BF16),
            pltpu.VMEM((SIDE, N_SP, CAP, T), BF16),
            pltpu.VMEM((3, N_SP, CAP, T), BF16),
            pltpu.VMEM((N_SP, CAP, T), BF16),
            pltpu.VMEM((N_SP, CAP, T), BF16),
            pltpu.VMEM((N_TP, T, T), BF16),
            pltpu.VMEM((N_TP, T, T), BF16),
            pltpu.VMEM((T, T), F32),
            dma((9,)),
            dma((2,)),
            dma((2,)),
            dma((3,)),
            dma((3,)),
            dma,
            dma,
            dma,
            dma,
            dma,
            dma,
            dma,
            dma,
            dma,
            dma,
            dma,
            dma((CHUNKS,)),
            dma((STEPS * CHUNKS + 3,)),
            dma((STEPS * CHUNKS + 3,)),
            dma,
            dma,
            dma,
            dma,
        ],
        compiler_params=pltpu.CompilerParams(collective_id=0, has_side_effects=True),
    )(
        stream,
        values_in,
        in_gate,
        out_gate,
        documents[None, :],
        conv_taps,
        head_gain[None, :],
        mix_weight,
        norm_gain[None, :],
        routes.T,
        route_weight.T,
        expert_gate,
        expert_up,
        expert_down.reshape(SIDE, SIDE, T, T),
        shared_gate,
        shared_up,
        shared_down,
    )


def solution(mesh):
    in_specs = (
        P("tp", "sp"),
        P("tp", "sp"),
        P("tp", "sp"),
        P("tp", "sp"),
        P("sp"),
        P(None, "tp"),
        P("tp"),
        P("tp", None),
        P("tp"),
        P("sp", None),
        P("sp", None),
        P("sp", None, "tp"),
        P("sp", None, "tp"),
        P("sp", None, "tp"),
        P(None, "tp"),
        P(None, "tp"),
        P("tp", None),
    )
    return jax.shard_map(
        local, mesh=mesh, in_specs=in_specs, out_specs=P("tp", "sp"), check_vma=False
    )
```

```python
import jax
import jax.numpy as jnp
from jax import lax
from jax.experimental import pallas as pl
from jax.experimental.pallas import tpu as pltpu
from jax.sharding import PartitionSpec as P

F32 = jnp.float32
BF16 = jnp.bfloat16
MESH = pl.DeviceIdType.MESH
EPS = 1e-06

D = 2048
T = 128
HEAD = 64
N_SP = 32
N_TP = 16
N_Z = 16
SIDE = 4
CAP = 24
TOP_K = 4
SLOTS = N_SP * CAP
DISTANCES = ((0, 1, -1, 2), (8, -7, 7, -6, 6, -5, 5, -4), (4, -3, 3, -2))
PLACES = [dz for chunk in DISTANCES for dz in chunk]
CHUNKS = len(DISTANCES)
SIZES = [2 * len(chunk) for chunk in DISTANCES]
STARTS = [sum(SIZES[:c]) for c in range(CHUNKS)]
DIRECT = (True, True, True)
STEPS = 5
LAG = 1.5
SHARED = ((1, 0), (1, 1), (1, 3))
SHARED_SEND_AFTER = (CHUNKS - 1, -2)


def dot(a, b, contract=((1,), (0,)), precision=None):
    return lax.dot_general(
        a, b, (contract, ((), ())), precision=precision, preferred_element_type=F32
    )


def iota(shape, dim):
    return lax.broadcasted_iota(jnp.int32, shape, dim)


def column_of(row, n):
    eye = iota((n, n), 0) == iota((n, n), 1)
    return jnp.sum(jnp.where(eye, jnp.broadcast_to(row, (n, n)), 0.0), axis=1, keepdims=True)


def kernel(
    stream_far,
    values_in_far,
    in_gate_far,
    out_gate_far,
    documents_far,
    conv_taps_far,
    head_gain_far,
    mix_weight,
    norm_gain_far,
    routes_far,
    route_weight_far,
    expert_gate,
    expert_up,
    expert_down,
    shared_gate,
    shared_up,
    shared_down,
    out,
    stream,
    values_in,
    in_gate,
    out_gate,
    documents,
    conv_taps,
    head_gain,
    norm_gain,
    routes,
    route_weight,
    halo_v,
    halo_g,
    halo_d,
    mix_here,
    mix_w,
    w_gu,
    w_down,
    w_one,
    w_two,
    s_gu,
    s_down,
    head_all,
    gains,
    normed_all,
    pick,
    comb_hi,
    comb_lo,
    disp_out,
    rows_all,
    mid_all,
    part,
    direct,
    ret_out,
    ret_in,
    sh_part,
    sh_in,
    hidden,
    told,
    load_sem,
    down_s,
    down_r,
    halo_s,
    halo_r,
    mix_s,
    mix_r,
    swap_s,
    swap_r,
    head_s,
    head_r,
    tail_s,
    tail_r,
    gain_s,
    gain_r,
    disp_s,
    disp_r,
    gat_s,
    gat_r,
    ret_s,
    ret_r,
    sh_s,
    sh_r,
):
    sp = lax.axis_index("sp")
    tp = lax.axis_index("tp")
    z, core = sp // 2, sp % 2
    y, x = tp // SIDE, tp % SIDE

    def remote(src, dst, send, recv, **where):
        return pltpu.make_async_remote_copy(
            src_ref=src,
            dst_ref=dst,
            send_sem=send,
            recv_sem=recv,
            device_id=where,
            device_id_type=MESH,
        )

    barrier = pltpu.get_barrier_semaphore()

    def along_z(dz, other):
        return 2 * ((z + dz + N_Z) % N_Z) + (core + other) % 2

    near = [(0, 1)] + [(dz, other) for dz in (-1, 1, -2, 2) for other in (0, 1)]
    for dz, other in near:
        pl.semaphore_signal(
            barrier, inc=1, device_id={"sp": along_z(dz, other)}, device_id_type=MESH
        )

    @pl.loop(1, N_TP)
    def _(step):
        pl.semaphore_signal(
            barrier, inc=1, device_id={"tp": (tp + step) % N_TP}, device_id_type=MESH
        )

    loads = [
        pltpu.make_async_copy(src, dst, load_sem.at[i])
        for i, (src, dst) in enumerate(
            [
                (routes_far, routes),
                (route_weight_far, route_weight),
                (values_in_far, values_in),
                (in_gate_far, in_gate),
                (documents_far, documents),
                (out_gate_far, out_gate),
                (conv_taps_far, conv_taps),
                (head_gain_far, head_gain),
                (norm_gain_far, norm_gain),
                (stream_far, stream),
                (mix_weight, mix_here),
                (expert_down, w_down),
                (expert_down.at[y], w_one.at[y]),
                (expert_down.at[:, x], w_two.at[x]),
                (shared_gate, s_gu.at[:, pl.ds(0, T)]),
                (shared_up, s_gu.at[:, pl.ds(T, T)]),
                (shared_down, s_down),
                (expert_gate.at[0], w_gu.at[:, pl.ds(0, T)]),
                (expert_up.at[0], w_gu.at[:, pl.ds(T, T)]),
            ]
        )
    ]
    for load in loads:
        load.start()
    small, loads = loads[:10], loads[10:]

    for load in small[:2]:
        load.wait()
    line = iota((T, T), 0)
    named = jnp.zeros((T, T), F32)
    weight = jnp.zeros((T, T), F32)
    for k in range(TOP_K):
        hit = routes[k : k + 1, :] == line
        named = jnp.where(hit, 1.0, named)
        weight = jnp.where(hit, route_weight[k : k + 1, :], weight)
    before = jnp.where(line < iota((T, T), 1), 1.0, 0.0).astype(BF16)
    earlier = dot(named.astype(BF16), before)
    slot = jnp.where(named > 0, earlier, 200.0)
    slot_t = slot.T.astype(BF16)
    slot = slot.astype(BF16)
    weight = weight.T

    def slot_number(shape, dim):
        number = iota(shape, dim).astype(F32)
        return number - CAP * jnp.floor((number + 0.5) * (1.0 / CAP))

    away = iota((SLOTS, T), 0) - CAP * iota((SLOTS, T), 1)
    owner = jnp.where((away >= 0) & (away < CAP), 1.0, 0.0).astype(BF16)
    taken = dot(owner, slot)
    pick[...] = jnp.where(taken == slot_number((SLOTS, T), 0), 1.0, 0.0).astype(BF16)
    away = iota((T, SLOTS), 1) - CAP * iota((T, SLOTS), 0)
    owner = jnp.where((away >= 0) & (away < CAP), 1.0, 0.0).astype(BF16)
    taken = dot(slot_t, owner) == slot_number((T, SLOTS), 1)
    weight_hi = weight.astype(BF16)
    weight_lo = (weight - weight_hi.astype(F32)).astype(BF16)
    comb_hi[...] = jnp.where(taken, dot(weight_hi, owner), 0.0).astype(BF16)
    comb_lo[...] = jnp.where(taken, dot(weight_lo, owner), 0.0).astype(BF16)

    pl.semaphore_wait(barrier, N_TP - 1 + len(near))

    def tell(step):
        for dz in (-2 << step, 2 << step):
            pl.semaphore_signal(
                told.at[step], inc=1, device_id={"sp": along_z(dz, 0)}, device_id_type=MESH
            )

    tell(0)

    for load in small[2:]:
        load.wait()

    behind = (sp + 1) % N_SP
    halos = [
        remote(src, dst, halo_s.at[i], halo_r.at[i], sp=behind)
        for i, (src, dst) in enumerate(
            [(values_in, halo_v), (in_gate, halo_g), (documents, halo_d)]
        )
    ]
    for halo in halos:
        halo.start()

    def arrive(ref, recv):
        remote(ref, ref, recv, recv, sp=behind).wait_recv()

    def leave(ref, send):
        remote(ref, ref, send, send, sp=behind).wait_send()

    def to_plane(src_of, dst, send, recv):
        @pl.loop(1, N_TP)
        def _(step):
            peer = (tp + step) % N_TP
            remote(src_of(peer), dst, send, recv, tp=peer).start()

    rows = pl.ds(pl.multiple_of(core * (HEAD // 2), HEAD // 2), HEAD // 2)

    def columns(peer):
        return mix_here.at[rows, pl.ds(pl.multiple_of(peer * T, T), T)]

    loads[0].wait()
    to_plane(columns, mix_w.at[tp, rows], mix_s, mix_r)
    mix_w[tp, rows] = mix_here[rows, pl.ds(pl.multiple_of(tp * T, T), T)]

    product = values_in[...].astype(F32) * in_gate[...].astype(F32)
    docs = jnp.broadcast_to(documents[...], (8, T))
    tap = [column_of(conv_taps[j : j + 1, :], HEAD) for j in range(3)]
    gain_col = column_of(head_gain[...], HEAD)

    def heads_after(product_before, docs_before):
        convolved = jnp.zeros((HEAD, T), F32)
        for j in range(3):
            back = 2 - j
            if back:
                shifted = jnp.where(
                    iota((HEAD, T), 1) < back,
                    pltpu.roll(product_before, back, 1),
                    pltpu.roll(product, back, 1),
                )
                docs_then = jnp.where(
                    iota((8, T), 1) < back,
                    pltpu.roll(docs_before, back, 1),
                    pltpu.roll(docs, back, 1),
                )
                same = jnp.where(docs_then == docs, 1.0, 0.0)[0:1, :]
                convolved = convolved + tap[j] * shifted * same
            else:
                convolved = convolved + tap[j] * product
        mixed = out_gate[...].astype(F32) * convolved
        spread = jnp.mean(mixed * mixed, axis=0, keepdims=True)
        heads = (mixed * lax.rsqrt(spread + EPS) * gain_col).T
        return jnp.concatenate([heads[:HEAD], heads[HEAD:]], axis=1).astype(BF16)

    first, rest = pl.ds(0, 8), pl.ds(8, HEAD - 8)
    head_all[tp, rest] = heads_after(product, docs)[8:]
    to_plane(lambda peer: head_all.at[tp, rest], head_all.at[tp, rest], head_s, head_r)
    for halo in halos:
        halo.wait_recv()
    product_before = halo_v[...].astype(F32) * halo_g[...].astype(F32)
    docs_before = jnp.where(sp == 0, -1, jnp.broadcast_to(halo_d[...], (8, T)))
    head_all[tp, first] = heads_after(product_before, docs_before)[:8]
    to_plane(lambda peer: head_all.at[tp, first], head_all.at[tp, first], tail_s, tail_r)

    pl.semaphore_wait(told.at[0], 2)
    tell(1)

    others = pl.ds(0, N_TP - 1)
    arrive(mix_w.at[others, pl.ds(0, HEAD // 2)], mix_r)
    swap = remote(mix_w.at[:, rows], mix_w.at[:, rows], swap_s, swap_r, sp=2 * z + 1 - core)
    swap.start()
    for load in loads[1:4]:
        load.wait()
    for way in (2, -1, 1):
        beside_y, beside_x = (y + way + SIDE) % SIDE, (x + way + SIDE) % SIDE
        remote(
            w_down.at[beside_y], w_one.at[y], down_s.at[0], down_r.at[0], tp=SIDE * beside_y + x
        ).start()
        remote(
            w_down.at[:, beside_x], w_two.at[x], down_s.at[1], down_r.at[1], tp=SIDE * y + beside_x
        ).start()

    total = stream[...].astype(F32).T
    swap.wait_recv()
    arrive(head_all.at[others, rest], head_r)
    arrive(head_all.at[others, first], tail_r)
    all_heads = jnp.concatenate([head_all[j] for j in range(N_TP)], axis=1)
    none = jnp.zeros((HEAD, T), BF16)
    early = jnp.concatenate([v for j in range(N_TP) for v in (mix_w[j], none)], axis=0)
    late = jnp.concatenate([v for j in range(N_TP) for v in (none, mix_w[j])], axis=0)
    mixer = dot(all_heads, jnp.concatenate([early, late], axis=1))
    total = total + jnp.concatenate([mixer[:, :T], mixer[:, T:]], axis=0)
    hidden[...] = total
    normed = (total * norm_gain[...]).astype(BF16)

    normed_all[y, x] = normed
    disp_out[...] = dot(pick[...], normed).astype(BF16).reshape(N_SP, CAP, T)
    order = [(dz, other) for dz in PLACES for other in (0, 1)][1:]

    def disp_copy(dz, other):
        place = PLACES.index(dz)
        expert = 2 * ((z - dz + N_Z) % N_Z) + ((core + 1 + other) % 2 if dz else 1 - core)
        block = 2 * place + core
        return remote(
            disp_out.at[expert],
            rows_all.at[y, x, block],
            disp_s,
            disp_r.at[next(c for c in range(CHUNKS) if dz in DISTANCES[c])],
            sp=expert,
        )

    for dz, other in order:
        if dz in DISTANCES[0]:
            disp_copy(dz, other).start()
    own = core
    rows_all[y, x, own] = disp_out[sp]

    def wait_disp(chunk):
        count = SIZES[chunk] - (chunk == 0)
        arrive(rows_all.at[y, x, pl.ds(STARTS[chunk], count)], disp_r.at[chunk])

    def at_x(way):
        return (x + way + SIDE) % SIDE

    def at_y(way):
        return (y + way + SIDE) % SIDE

    to_x = [SIDE * y + at_x(-1), SIDE * y + at_x(1)]
    to_y = [SIDE * at_y(-1) + x, SIDE * at_y(1) + x]
    ways = (-1, 1)

    def numbered(moves, index):
        return [
            remote(src, dst, gat_s.at[index], gat_r.at[index], tp=peer) for src, dst, peer in moves
        ]

    to_x.append(SIDE * y + at_x(2))
    to_y.append(SIDE * at_y(2) + x)

    def gather_copies(buf, start, size, index, stage, short):
        both = pl.ds(start, size)
        one, two = pl.ds(start, size // 2), pl.ds(start + size // 2, size // 2)
        a, b = pl.ds(start, size // 4), pl.ds(start + size // 4, size // 4)
        c, d = pl.ds(start + size // 2, size // 4), pl.ds(start + size // 2 + size // 4, size // 4)
        if stage == 0:
            moves = [(buf.at[y, x, both], to[i]) for i in (2, 0, 1) for to in (to_x, to_y)]
        elif stage == 1:
            moves = []
            for way in (-1, 1, 2):
                for i in (2, 0, 1) if short else (0, 1):
                    moves += [(buf.at[y, at_x(way), one], to_y[i]), (buf.at[at_y(way), x, two], to_x[i])]
        else:
            moves = [
                (buf.at[at_y(-1), at_x(1), one], to_y[1]),
                (buf.at[at_y(1), at_x(-1), two], to_x[1]),
                (buf.at[at_y(1), at_x(-1), one], to_y[0]),
                (buf.at[at_y(-1), at_x(1), two], to_x[0]),
                (buf.at[at_y(-1), at_x(2), a], to_y[1]),
                (buf.at[at_y(2), at_x(-1), c], to_x[1]),
                (buf.at[at_y(1), at_x(2), b], to_y[0]),
                (buf.at[at_y(2), at_x(1), d], to_x[0]),
            ]
        return numbered([(ref, ref, peer) for ref, peer in moves], index)

    def thirds(stage, short):
        return (2, 3 if short else 2, 1)[stage]

    def row_copies(chunk, stage):
        index = STEPS * chunk + stage
        start, size, short = STARTS[chunk], SIZES[chunk], DIRECT[chunk]
        copies = lambda: gather_copies(rows_all, start, size, index, stage, short)
        count = thirds(stage, DIRECT[chunk])
        return copies, rows_all.at[pl.ds(0, count), pl.ds(0, 3), pl.ds(0, SIZES[chunk])], index

    def normed_copies(stage):
        index = STEPS * CHUNKS + stage
        copies = lambda: gather_copies(normed_all, 0, T, index, stage, False)
        return copies, normed_all.at[pl.ds(0, thirds(stage, False)), pl.ds(0, 3)], index

    def expert_copies(chunk, stage):
        size = SIZES[chunk] // 2
        one, two = pl.ds(STARTS[chunk], size), pl.ds(STARTS[chunk] + size, size)
        moves = []
        for i, way in ((2, 2), (0, -1), (1, 1)):
            if stage == 0:
                moves.append((mid_all.at[y, x, one], mid_all.at[y, x, one], to_x[i]))
                moves.append((mid_all.at[y, x, two], mid_all.at[y, x, two], to_y[i]))
            else:
                moves.append((part.at[at_y(way), one], direct.at[i, one], to_y[i]))
                moves.append((part.at[at_x(way), two], direct.at[i, two], to_x[i]))
        index = STEPS * chunk + 3 + stage
        return lambda: numbered(moves, index), direct.at[:, pl.ds(0, SIZES[chunk])], index

    def go(kind):
        for copy in kind[0]():
            copy.start()

    def got(kind):
        arrive(kind[1], gat_r.at[kind[2]])

    def rows_of(ref):
        return ref.reshape(ref.shape[0] * CAP, T)

    def silu(v):
        return v / (1.0 + jnp.exp(-v))

    def gated(blocks, weights):
        squares = jnp.zeros(blocks[0].shape, F32)
        for j, block in enumerate(blocks):
            wide = block.astype(F32)
            squares = squares + wide * wide * (1.0 / (gains[j] * gains[j]))
        scale = lax.rsqrt(jnp.sum(squares, axis=1, keepdims=True) / D + EPS)
        pair = dot(jnp.concatenate(blocks, axis=1), weights) * scale
        return (silu(pair[:, :T]) * pair[:, T:]).astype(BF16)

    def gate_up(chunk):
        here = pl.ds(STARTS[chunk], SIZES[chunk])
        blocks = [rows_of(rows_all[i, j, here]) for i in range(SIDE) for j in range(SIDE)]
        mid = gated(blocks, w_gu[...])
        mid_all[y, x, here] = mid.reshape(SIZES[chunk], CAP, T)

    def down(chunk):
        size = SIZES[chunk] // 2
        for half in range(2):
            here = pl.ds(STARTS[chunk] + size * half, size)
            line = [mid_all[y, k, here] if half == 0 else mid_all[k, x, here] for k in range(SIDE)]
            line = jnp.concatenate([rows_of(block) for block in line], axis=1)
            weights = w_two if half else w_one
            for q in range(0, SIDE, 2):
                pair = jnp.concatenate(
                    [weights[q + n].reshape(SIDE * T, T) for n in range(2)], axis=1
                )
                result = dot(line, pair).astype(BF16)
                for n in range(2):
                    part[q + n, here] = result[:, n * T : (n + 1) * T].reshape(size, CAP, T)

    def finish(chunk):
        size = SIZES[chunk] // 2
        for half in range(2):
            here = pl.ds(STARTS[chunk] + size * half, size)
            value = part[x if half else y, here].astype(F32)
            for i in range(3):
                value = value + direct[i, here].astype(F32)
            ret_out[here] = value.astype(BF16)

    def ret_copy(dz, other):
        place = PLACES.index(dz)
        group_core = (core + 1 + other) % 2 if dz else 1 - core
        group = 2 * ((z + dz + N_Z) % N_Z) + group_core
        return remote(
            ret_out.at[2 * place + group_core],
            ret_in.at[sp],
            ret_s,
            ret_r,
            sp=group,
        )

    def start_ret(chunk):
        for dz, other in order:
            if dz in DISTANCES[chunk]:
                ret_copy(dz, other).start()

    def shared_expert():
        for load in loads[4:7]:
            load.wait()
        mid = gated([normed_all[i, j] for i in range(SIDE) for j in range(SIDE)], s_gu[...])
        for j in range(N_TP // 2):
            part = dot(mid, s_down[:, 2 * T * j : 2 * T * (j + 1)]).astype(BF16)
            sh_part[2 * j] = part[:, :T]
            sh_part[2 * j + 1] = part[:, T:]

    def row_stages(chunk):
        return 2 if DIRECT[chunk] else 3

    def advance(chunk, stage):
        rows = row_stages(chunk)
        if stage == 0:
            wait_disp(chunk)
            go(row_copies(chunk, 0))
        elif stage < rows:
            got(row_copies(chunk, stage - 1))
            go(row_copies(chunk, stage))
        elif stage == rows:
            got(row_copies(chunk, rows - 1))
            gate_up(chunk)
            go(expert_copies(chunk, 0))
        elif stage == rows + 1:
            got(expert_copies(chunk, 0))
            down(chunk)
            go(expert_copies(chunk, 1))
        else:
            got(expert_copies(chunk, 1))
            finish(chunk)
            start_ret(chunk)

    go(normed_copies(0))
    pl.semaphore_wait(told.at[1], 2)
    for dz, other in order:
        if dz not in DISTANCES[0]:
            disp_copy(dz, other).start()
    to_plane(lambda peer: norm_gain, gains.at[tp], gain_s, gain_r)
    gains[tp] = norm_gain[...]
    steps = sorted(
        (stage + LAG * chunk, chunk, stage)
        for chunk in range(CHUNKS)
        for stage in range(row_stages(chunk) + 3)
    )
    for _, chunk, stage in steps:
        left = stage - row_stages(chunk) - 3
        if (chunk, left) == (0, -3):
            arrive(gains.at[others], gain_r)
            for load in loads[7:]:
                load.wait()
        if (chunk, left) == (0, -2):
            arrive(w_one.at[pl.ds(0, 3)], down_r.at[0])
            arrive(w_two.at[pl.ds(0, 3)], down_r.at[1])
        advance(chunk, stage)
        for turn, after in enumerate(SHARED):
            if after == (chunk, stage):
                got(normed_copies(turn))
                if turn < 2:
                    go(normed_copies(turn + 1))
                else:
                    shared_expert()
                    sh_in[tp] = sh_part[tp]
        if (chunk, left) == SHARED_SEND_AFTER:
            to_plane(lambda peer: sh_part.at[peer], sh_in.at[tp], sh_s, sh_r)
        if (chunk, left) == (0, -1):
            ret_in[sp] = ret_out[own]

    arrive(sh_in.at[others], sh_r)
    total = hidden[...]
    for j in range(N_TP):
        total = total + sh_in[j].astype(F32)

    for halo in halos:
        halo.wait_send()
    swap.wait_send()
    for ref, send in (
        (mix_w.at[others, pl.ds(0, HEAD // 2)], mix_s),
        (head_all.at[others, rest], head_s),
        (head_all.at[others, first], tail_s),
        (gains.at[others], gain_s),
        (w_one.at[pl.ds(0, 3)], down_s.at[0]),
        (w_two.at[pl.ds(0, 3)], down_s.at[1]),
        (disp_out.at[pl.ds(0, N_SP - 1)], disp_s),
        (sh_in.at[others], sh_s),
    ):
        leave(ref, send)
    kinds = [normed_copies(stage) for stage in range(3)]
    for chunk in range(CHUNKS):
        kinds += [row_copies(chunk, stage) for stage in range(row_stages(chunk))]
        kinds += [expert_copies(chunk, stage) for stage in range(2)]
    for _, ref, index in kinds:
        leave(ref, gat_s.at[index])

    arrive(ret_in.at[pl.ds(0, N_SP - 1)], ret_r)
    returned = ret_in[...].reshape(SLOTS, T)
    total = total + dot(comb_hi[...], returned) + dot(comb_lo[...], returned)
    out[...] = total.T.astype(BF16)
    leave(ret_in.at[pl.ds(0, N_SP - 1)], ret_s)


def local(
    stream,
    values_in,
    in_gate,
    out_gate,
    documents,
    conv_taps,
    head_gain,
    mix_weight,
    norm_gain,
    routes,
    route_weight,
    expert_gate,
    expert_up,
    expert_down,
    shared_gate,
    shared_up,
    shared_down,
):
    vmem = pl.BlockSpec(memory_space=pltpu.VMEM)
    hbm = pl.BlockSpec(memory_space=pl.ANY)
    dma = pltpu.SemaphoreType.DMA
    return pl.pallas_call(
        kernel,
        name="layer",
        out_shape=jax.ShapeDtypeStruct((T, T), BF16),
        in_specs=[hbm] * 17,
        out_specs=vmem,
        scratch_shapes=[
            pltpu.VMEM((T, T), BF16),
            pltpu.VMEM((HEAD, T), BF16),
            pltpu.VMEM((HEAD, T), BF16),
            pltpu.VMEM((HEAD, T), BF16),
            pltpu.VMEM((1, T), jnp.int32),
            pltpu.VMEM((3, HEAD), F32),
            pltpu.VMEM((1, HEAD), F32),
            pltpu.VMEM((1, T), F32),
            pltpu.VMEM((TOP_K, T), jnp.int32),
            pltpu.VMEM((TOP_K, T), F32),
            pltpu.VMEM((HEAD, T), BF16),
            pltpu.VMEM((HEAD, T), BF16),
            pltpu.VMEM((1, T), jnp.int32),
            pltpu.VMEM((HEAD, D), BF16),
            pltpu.VMEM((N_TP, HEAD, T), BF16),
            pltpu.VMEM((D, 2 * T), BF16),
            pltpu.VMEM((SIDE, SIDE, T, T), BF16),
            pltpu.VMEM((SIDE, SIDE, T, T), BF16),
            pltpu.VMEM((SIDE, SIDE, T, T), BF16),
            pltpu.VMEM((D, 2 * T), BF16),
            pltpu.VMEM((T, D), BF16),
            pltpu.VMEM((N_TP, HEAD, T), BF16),
            pltpu.VMEM((N_TP, 1, T), F32),
            pltpu.VMEM((SIDE, SIDE, T, T), BF16),
            pltpu.VMEM((SLOTS, T), BF16),
            pltpu.VMEM((T, SLOTS), BF16),
            pltpu.VMEM((T, SLOTS), BF16),
            pltpu.VMEM((N_SP, CAP, T), BF16),
            pltpu.VMEM((SIDE, SIDE, N_SP, CAP, T), BF16),
            pltpu.VMEM((SIDE, SIDE, N_SP, CAP, T), BF16),
            pltpu.VMEM((SIDE, N_SP, CAP, T), BF16),
            pltpu.VMEM((3, N_SP, CAP, T), BF16),
            pltpu.VMEM((N_SP, CAP, T), BF16),
            pltpu.VMEM((N_SP, CAP, T), BF16),
            pltpu.VMEM((N_TP, T, T), BF16),
            pltpu.VMEM((N_TP, T, T), BF16),
            pltpu.VMEM((T, T), F32),
            pltpu.SemaphoreType.REGULAR((2,)),
            dma((19,)),
            dma((2,)),
            dma((2,)),
            dma((3,)),
            dma((3,)),
            dma,
            dma,
            dma,
            dma,
            dma,
            dma,
            dma,
            dma,
            dma,
            dma,
            dma,
            dma((CHUNKS,)),
            dma((STEPS * CHUNKS + 3,)),
            dma((STEPS * CHUNKS + 3,)),
            dma,
            dma,
            dma,
            dma,
        ],
        compiler_params=pltpu.CompilerParams(collective_id=0, has_side_effects=True),
    )(
        stream,
        values_in,
        in_gate,
        out_gate,
        documents[None, :],
        conv_taps,
        head_gain[None, :],
        mix_weight,
        norm_gain[None, :],
        routes.T,
        route_weight.T,
        expert_gate,
        expert_up,
        expert_down.reshape(SIDE, SIDE, T, T),
        shared_gate,
        shared_up,
        shared_down,
    )


def solution(mesh):
    in_specs = (
        P("tp", "sp"),
        P("tp", "sp"),
        P("tp", "sp"),
        P("tp", "sp"),
        P("sp"),
        P(None, "tp"),
        P("tp"),
        P("tp", None),
        P("tp"),
        P("sp", None),
        P("sp", None),
        P("sp", None, "tp"),
        P("sp", None, "tp"),
        P("sp", None, "tp"),
        P(None, "tp"),
        P(None, "tp"),
        P("tp", None),
    )
    return jax.shard_map(
        local, mesh=mesh, in_specs=in_specs, out_specs=P("tp", "sp"), check_vma=False
    )
```

```python
import jax
import jax.numpy as jnp
from jax import lax
from jax.experimental import pallas as pl
from jax.experimental.pallas import tpu as pltpu
from jax.sharding import PartitionSpec as P

F32 = jnp.float32
BF16 = jnp.bfloat16
MESH = pl.DeviceIdType.MESH
EPS = 1e-06

D = 2048
T = 128
HEAD = 64
N_SP = 32
N_TP = 16
N_Z = 16
SIDE = 4
CAP = 24
TOP_K = 4
SLOTS = N_SP * CAP
DISTANCES = ((0, 1, -1, 2), (8, -7, 7, -6, 6, -5, 5, -4), (4, -3, 3, -2))
PLACES = [dz for chunk in DISTANCES for dz in chunk]
CHUNKS = len(DISTANCES)
SIZES = [2 * len(chunk) for chunk in DISTANCES]
STARTS = [sum(SIZES[:c]) for c in range(CHUNKS)]
DIRECT = (True, True, True)
STEPS = 5
LAG = 1.99
SHARED = ((0, 1), (0, 2), (1, 2))
SHARED_SEND_AFTER = (CHUNKS - 1, -2)


def dot(a, b, contract=((1,), (0,)), precision=None):
    return lax.dot_general(
        a, b, (contract, ((), ())), precision=precision, preferred_element_type=F32
    )


def iota(shape, dim):
    return lax.broadcasted_iota(jnp.int32, shape, dim)


def column_of(row, n):
    eye = iota((n, n), 0) == iota((n, n), 1)
    return jnp.sum(jnp.where(eye, jnp.broadcast_to(row, (n, n)), 0.0), axis=1, keepdims=True)


def kernel(
    stream_far,
    values_in_far,
    in_gate_far,
    out_gate_far,
    documents_far,
    conv_taps_far,
    head_gain_far,
    mix_weight,
    norm_gain_far,
    routes_far,
    route_weight_far,
    expert_gate,
    expert_up,
    expert_down,
    shared_gate,
    shared_up,
    shared_down,
    out,
    stream,
    values_in,
    in_gate,
    out_gate,
    documents,
    conv_taps,
    head_gain,
    norm_gain,
    routes,
    route_weight,
    halo_v,
    halo_g,
    halo_d,
    mix_here,
    mix_w,
    w_gu,
    w_down,
    w_one,
    w_two,
    s_gu,
    s_down,
    head_all,
    gains,
    normed_all,
    pick,
    comb_hi,
    comb_lo,
    disp_out,
    rows_all,
    mid_all,
    part,
    direct,
    ret_out,
    ret_in,
    sh_part,
    sh_in,
    hidden,
    told,
    load_sem,
    down_s,
    down_r,
    halo_s,
    halo_r,
    mix_s,
    mix_r,
    swap_s,
    swap_r,
    head_s,
    head_r,
    tail_s,
    tail_r,
    gain_s,
    gain_r,
    disp_s,
    disp_r,
    gat_s,
    gat_r,
    ret_s,
    ret_r,
    sh_s,
    sh_r,
):
    sp = lax.axis_index("sp")
    tp = lax.axis_index("tp")
    z, core = sp // 2, sp % 2
    y, x = tp // SIDE, tp % SIDE

    def remote(src, dst, send, recv, **where):
        return pltpu.make_async_remote_copy(
            src_ref=src,
            dst_ref=dst,
            send_sem=send,
            recv_sem=recv,
            device_id=where,
            device_id_type=MESH,
        )

    barrier = pltpu.get_barrier_semaphore()

    def along_z(dz, other):
        return 2 * ((z + dz + N_Z) % N_Z) + (core + other) % 2

    near = [(0, 1)] + [(dz, other) for dz in (-1, 1, -2, 2) for other in (0, 1)]
    for dz, other in near:
        pl.semaphore_signal(
            barrier, inc=1, device_id={"sp": along_z(dz, other)}, device_id_type=MESH
        )

    @pl.loop(1, N_TP)
    def _(step):
        pl.semaphore_signal(
            barrier, inc=1, device_id={"tp": (tp + step) % N_TP}, device_id_type=MESH
        )

    loads = [
        pltpu.make_async_copy(src, dst, load_sem.at[i])
        for i, (src, dst) in enumerate(
            [
                (routes_far, routes),
                (route_weight_far, route_weight),
                (values_in_far, values_in),
                (in_gate_far, in_gate),
                (documents_far, documents),
                (out_gate_far, out_gate),
                (conv_taps_far, conv_taps),
                (head_gain_far, head_gain),
                (norm_gain_far, norm_gain),
                (stream_far, stream),
                (mix_weight, mix_here),
                (expert_down, w_down),
                (expert_down.at[y], w_one.at[y]),
                (expert_down.at[:, x], w_two.at[x]),
                (shared_gate, s_gu.at[:, pl.ds(0, T)]),
                (shared_up, s_gu.at[:, pl.ds(T, T)]),
                (shared_down, s_down),
                (expert_gate.at[0], w_gu.at[:, pl.ds(0, T)]),
                (expert_up.at[0], w_gu.at[:, pl.ds(T, T)]),
            ]
        )
    ]
    for load in loads:
        load.start()
    small, loads = loads[:10], loads[10:]

    for load in small[:2]:
        load.wait()
    line = iota((T, T), 0)
    named = jnp.zeros((T, T), F32)
    weight = jnp.zeros((T, T), F32)
    for k in range(TOP_K):
        hit = routes[k : k + 1, :] == line
        named = jnp.where(hit, 1.0, named)
        weight = jnp.where(hit, route_weight[k : k + 1, :], weight)
    before = jnp.where(line < iota((T, T), 1), 1.0, 0.0).astype(BF16)
    earlier = dot(named.astype(BF16), before)
    slot = jnp.where(named > 0, earlier, 200.0)
    slot_t = slot.T.astype(BF16)
    slot = slot.astype(BF16)
    weight = weight.T

    def slot_number(shape, dim):
        number = iota(shape, dim).astype(F32)
        return number - CAP * jnp.floor((number + 0.5) * (1.0 / CAP))

    away = iota((SLOTS, T), 0) - CAP * iota((SLOTS, T), 1)
    owner = jnp.where((away >= 0) & (away < CAP), 1.0, 0.0).astype(BF16)
    taken = dot(owner, slot)
    pick[...] = jnp.where(taken == slot_number((SLOTS, T), 0), 1.0, 0.0).astype(BF16)
    away = iota((T, SLOTS), 1) - CAP * iota((T, SLOTS), 0)
    owner = jnp.where((away >= 0) & (away < CAP), 1.0, 0.0).astype(BF16)
    taken = dot(slot_t, owner) == slot_number((T, SLOTS), 1)
    weight_hi = weight.astype(BF16)
    weight_lo = (weight - weight_hi.astype(F32)).astype(BF16)
    comb_hi[...] = jnp.where(taken, dot(weight_hi, owner), 0.0).astype(BF16)
    comb_lo[...] = jnp.where(taken, dot(weight_lo, owner), 0.0).astype(BF16)

    pl.semaphore_wait(barrier, N_TP - 1 + len(near))

    def tell(step):
        for dz in (-2 << step, 2 << step):
            pl.semaphore_signal(
                told.at[step], inc=1, device_id={"sp": along_z(dz, 0)}, device_id_type=MESH
            )

    tell(0)

    for load in small[2:]:
        load.wait()

    behind = (sp + 1) % N_SP
    halos = [
        remote(src, dst, halo_s.at[i], halo_r.at[i], sp=behind)
        for i, (src, dst) in enumerate(
            [(values_in, halo_v), (in_gate, halo_g), (documents, halo_d)]
        )
    ]
    for halo in halos:
        halo.start()

    def arrive(ref, recv):
        remote(ref, ref, recv, recv, sp=behind).wait_recv()

    def leave(ref, send):
        remote(ref, ref, send, send, sp=behind).wait_send()

    def to_plane(src_of, dst, send, recv):
        @pl.loop(1, N_TP)
        def _(step):
            peer = (tp + step) % N_TP
            remote(src_of(peer), dst, send, recv, tp=peer).start()

    rows = pl.ds(pl.multiple_of(core * (HEAD // 2), HEAD // 2), HEAD // 2)

    def columns(peer):
        return mix_here.at[rows, pl.ds(pl.multiple_of(peer * T, T), T)]

    loads[0].wait()
    to_plane(columns, mix_w.at[tp, rows], mix_s, mix_r)
    mix_w[tp, rows] = mix_here[rows, pl.ds(pl.multiple_of(tp * T, T), T)]

    product = values_in[...].astype(F32) * in_gate[...].astype(F32)
    docs = jnp.broadcast_to(documents[...], (8, T))
    tap = [column_of(conv_taps[j : j + 1, :], HEAD) for j in range(3)]
    gain_col = column_of(head_gain[...], HEAD)

    def heads_after(product_before, docs_before):
        convolved = jnp.zeros((HEAD, T), F32)
        for j in range(3):
            back = 2 - j
            if back:
                shifted = jnp.where(
                    iota((HEAD, T), 1) < back,
                    pltpu.roll(product_before, back, 1),
                    pltpu.roll(product, back, 1),
                )
                docs_then = jnp.where(
                    iota((8, T), 1) < back,
                    pltpu.roll(docs_before, back, 1),
                    pltpu.roll(docs, back, 1),
                )
                same = jnp.where(docs_then == docs, 1.0, 0.0)[0:1, :]
                convolved = convolved + tap[j] * shifted * same
            else:
                convolved = convolved + tap[j] * product
        mixed = out_gate[...].astype(F32) * convolved
        spread = jnp.mean(mixed * mixed, axis=0, keepdims=True)
        heads = (mixed * lax.rsqrt(spread + EPS) * gain_col).T
        return jnp.concatenate([heads[:HEAD], heads[HEAD:]], axis=1).astype(BF16)

    first, rest = pl.ds(0, 8), pl.ds(8, HEAD - 8)
    head_all[tp, rest] = heads_after(product, docs)[8:]
    to_plane(lambda peer: head_all.at[tp, rest], head_all.at[tp, rest], head_s, head_r)
    for halo in halos:
        halo.wait_recv()
    product_before = halo_v[...].astype(F32) * halo_g[...].astype(F32)
    docs_before = jnp.where(sp == 0, -1, jnp.broadcast_to(halo_d[...], (8, T)))
    head_all[tp, first] = heads_after(product_before, docs_before)[:8]
    to_plane(lambda peer: head_all.at[tp, first], head_all.at[tp, first], tail_s, tail_r)

    pl.semaphore_wait(told.at[0], 2)
    tell(1)

    others = pl.ds(0, N_TP - 1)
    arrive(mix_w.at[others, pl.ds(0, HEAD // 2)], mix_r)
    swap = remote(mix_w.at[:, rows], mix_w.at[:, rows], swap_s, swap_r, sp=2 * z + 1 - core)
    swap.start()
    for load in loads[1:4]:
        load.wait()
    for way in (2, -1, 1):
        beside_y, beside_x = (y + way + SIDE) % SIDE, (x + way + SIDE) % SIDE
        remote(
            w_down.at[beside_y], w_one.at[y], down_s.at[0], down_r.at[0], tp=SIDE * beside_y + x
        ).start()
        remote(
            w_down.at[:, beside_x], w_two.at[x], down_s.at[1], down_r.at[1], tp=SIDE * y + beside_x
        ).start()

    total = stream[...].astype(F32).T
    swap.wait_recv()
    arrive(head_all.at[others, rest], head_r)
    arrive(head_all.at[others, first], tail_r)
    all_heads = jnp.concatenate([head_all[j] for j in range(N_TP)], axis=1)
    none = jnp.zeros((HEAD, T), BF16)
    early = jnp.concatenate([v for j in range(N_TP) for v in (mix_w[j], none)], axis=0)
    late = jnp.concatenate([v for j in range(N_TP) for v in (none, mix_w[j])], axis=0)
    mixer = dot(all_heads, jnp.concatenate([early, late], axis=1))
    total = total + jnp.concatenate([mixer[:, :T], mixer[:, T:]], axis=0)
    hidden[...] = total
    normed = (total * norm_gain[...]).astype(BF16)

    normed_all[y, x] = normed
    disp_out[...] = dot(pick[...], normed).astype(BF16).reshape(N_SP, CAP, T)
    order = [(dz, other) for dz in PLACES for other in (0, 1)][1:]

    def disp_copy(dz, other):
        place = PLACES.index(dz)
        expert = 2 * ((z - dz + N_Z) % N_Z) + ((core + 1 + other) % 2 if dz else 1 - core)
        block = 2 * place + core
        return remote(
            disp_out.at[expert],
            rows_all.at[y, x, block],
            disp_s,
            disp_r.at[next(c for c in range(CHUNKS) if dz in DISTANCES[c])],
            sp=expert,
        )

    for dz, other in order:
        if dz in DISTANCES[0]:
            disp_copy(dz, other).start()
    own = core
    rows_all[y, x, own] = disp_out[sp]

    def wait_disp(chunk):
        count = SIZES[chunk] - (chunk == 0)
        arrive(rows_all.at[y, x, pl.ds(STARTS[chunk], count)], disp_r.at[chunk])

    def at_x(way):
        return (x + way + SIDE) % SIDE

    def at_y(way):
        return (y + way + SIDE) % SIDE

    to_x = [SIDE * y + at_x(-1), SIDE * y + at_x(1)]
    to_y = [SIDE * at_y(-1) + x, SIDE * at_y(1) + x]
    ways = (-1, 1)

    def numbered(moves, index):
        return [
            remote(src, dst, gat_s.at[index], gat_r.at[index], tp=peer) for src, dst, peer in moves
        ]

    to_x.append(SIDE * y + at_x(2))
    to_y.append(SIDE * at_y(2) + x)

    def gather_copies(buf, start, size, index, stage, short):
        both = pl.ds(start, size)
        one, two = pl.ds(start, size // 2), pl.ds(start + size // 2, size // 2)
        a, b = pl.ds(start, size // 4), pl.ds(start + size // 4, size // 4)
        c, d = pl.ds(start + size // 2, size // 4), pl.ds(start + size // 2 + size // 4, size // 4)
        if stage == 0:
            moves = [(buf.at[y, x, both], to[i]) for i in (2, 0, 1) for to in (to_x, to_y)]
        elif stage == 1:
            moves = []
            for way in (-1, 1, 2):
                for i in (2, 0, 1) if short else (0, 1):
                    moves += [(buf.at[y, at_x(way), one], to_y[i]), (buf.at[at_y(way), x, two], to_x[i])]
        else:
            moves = [
                (buf.at[at_y(-1), at_x(1), one], to_y[1]),
                (buf.at[at_y(1), at_x(-1), two], to_x[1]),
                (buf.at[at_y(1), at_x(-1), one], to_y[0]),
                (buf.at[at_y(-1), at_x(1), two], to_x[0]),
                (buf.at[at_y(-1), at_x(2), a], to_y[1]),
                (buf.at[at_y(2), at_x(-1), c], to_x[1]),
                (buf.at[at_y(1), at_x(2), b], to_y[0]),
                (buf.at[at_y(2), at_x(1), d], to_x[0]),
            ]
        return numbered([(ref, ref, peer) for ref, peer in moves], index)

    def thirds(stage, short):
        return (2, 3 if short else 2, 1)[stage]

    def row_copies(chunk, stage):
        index = STEPS * chunk + stage
        start, size, short = STARTS[chunk], SIZES[chunk], DIRECT[chunk]
        copies = lambda: gather_copies(rows_all, start, size, index, stage, short)
        count = thirds(stage, DIRECT[chunk])
        return copies, rows_all.at[pl.ds(0, count), pl.ds(0, 3), pl.ds(0, SIZES[chunk])], index

    def normed_copies(stage):
        index = STEPS * CHUNKS + stage
        copies = lambda: gather_copies(normed_all, 0, T, index, stage, False)
        return copies, normed_all.at[pl.ds(0, thirds(stage, False)), pl.ds(0, 3)], index

    def expert_copies(chunk, stage):
        size = SIZES[chunk] // 2
        one, two = pl.ds(STARTS[chunk], size), pl.ds(STARTS[chunk] + size, size)
        moves = []
        for i, way in ((2, 2), (0, -1), (1, 1)):
            if stage == 0:
                moves.append((mid_all.at[y, x, one], mid_all.at[y, x, one], to_x[i]))
                moves.append((mid_all.at[y, x, two], mid_all.at[y, x, two], to_y[i]))
            else:
                moves.append((part.at[at_y(way), one], direct.at[i, one], to_y[i]))
                moves.append((part.at[at_x(way), two], direct.at[i, two], to_x[i]))
        index = STEPS * chunk + 3 + stage
        return lambda: numbered(moves, index), direct.at[:, pl.ds(0, SIZES[chunk])], index

    def go(kind):
        for copy in kind[0]():
            copy.start()

    def got(kind):
        arrive(kind[1], gat_r.at[kind[2]])

    def rows_of(ref):
        return ref.reshape(ref.shape[0] * CAP, T)

    def silu(v):
        return v / (1.0 + jnp.exp(-v))

    def gated(blocks, weights):
        squares = jnp.zeros(blocks[0].shape, F32)
        for j, block in enumerate(blocks):
            wide = block.astype(F32)
            squares = squares + wide * wide * (1.0 / (gains[j] * gains[j]))
        scale = lax.rsqrt(jnp.sum(squares, axis=1, keepdims=True) / D + EPS)
        pair = dot(jnp.concatenate(blocks, axis=1), weights) * scale
        return (silu(pair[:, :T]) * pair[:, T:]).astype(BF16)

    def gate_up(chunk):
        here = pl.ds(STARTS[chunk], SIZES[chunk])
        blocks = [rows_of(rows_all[i, j, here]) for i in range(SIDE) for j in range(SIDE)]
        mid = gated(blocks, w_gu[...])
        mid_all[y, x, here] = mid.reshape(SIZES[chunk], CAP, T)

    def down(chunk):
        size = SIZES[chunk] // 2
        for half in range(2):
            here = pl.ds(STARTS[chunk] + size * half, size)
            line = [mid_all[y, k, here] if half == 0 else mid_all[k, x, here] for k in range(SIDE)]
            line = jnp.concatenate([rows_of(block) for block in line], axis=1)
            weights = w_two if half else w_one
            for q in range(0, SIDE, 2):
                pair = jnp.concatenate(
                    [weights[q + n].reshape(SIDE * T, T) for n in range(2)], axis=1
                )
                result = dot(line, pair).astype(BF16)
                for n in range(2):
                    part[q + n, here] = result[:, n * T : (n + 1) * T].reshape(size, CAP, T)

    def finish(chunk):
        size = SIZES[chunk] // 2
        for half in range(2):
            here = pl.ds(STARTS[chunk] + size * half, size)
            value = part[x if half else y, here].astype(F32)
            for i in range(3):
                value = value + direct[i, here].astype(F32)
            ret_out[here] = value.astype(BF16)

    def ret_copy(dz, other):
        place = PLACES.index(dz)
        group_core = (core + 1 + other) % 2 if dz else 1 - core
        group = 2 * ((z + dz + N_Z) % N_Z) + group_core
        return remote(
            ret_out.at[2 * place + group_core],
            ret_in.at[sp],
            ret_s,
            ret_r,
            sp=group,
        )

    def start_ret(chunk):
        for dz, other in order:
            if dz in DISTANCES[chunk]:
                ret_copy(dz, other).start()

    def shared_expert():
        for load in loads[4:7]:
            load.wait()
        mid = gated([normed_all[i, j] for i in range(SIDE) for j in range(SIDE)], s_gu[...])
        for j in range(N_TP // 2):
            part = dot(mid, s_down[:, 2 * T * j : 2 * T * (j + 1)]).astype(BF16)
            sh_part[2 * j] = part[:, :T]
            sh_part[2 * j + 1] = part[:, T:]

    def row_stages(chunk):
        return 2 if DIRECT[chunk] else 3

    def advance(chunk, stage):
        rows = row_stages(chunk)
        if stage == 0:
            wait_disp(chunk)
            go(row_copies(chunk, 0))
        elif stage < rows:
            got(row_copies(chunk, stage - 1))
            go(row_copies(chunk, stage))
        elif stage == rows:
            got(row_copies(chunk, rows - 1))
            gate_up(chunk)
            go(expert_copies(chunk, 0))
        elif stage == rows + 1:
            got(expert_copies(chunk, 0))
            down(chunk)
            go(expert_copies(chunk, 1))
        else:
            got(expert_copies(chunk, 1))
            finish(chunk)
            start_ret(chunk)

    go(normed_copies(0))
    pl.semaphore_wait(told.at[1], 2)
    for dz, other in order:
        if dz not in DISTANCES[0]:
            disp_copy(dz, other).start()
    to_plane(lambda peer: norm_gain, gains.at[tp], gain_s, gain_r)
    gains[tp] = norm_gain[...]
    steps = sorted(
        (stage + LAG * chunk, chunk, stage)
        for chunk in range(CHUNKS)
        for stage in range(row_stages(chunk) + 3)
    )
    for _, chunk, stage in steps:
        left = stage - row_stages(chunk) - 3
        if (chunk, left) == (0, -3):
            arrive(gains.at[others], gain_r)
            for load in loads[7:]:
                load.wait()
        if (chunk, left) == (0, -2):
            arrive(w_one.at[pl.ds(0, 3)], down_r.at[0])
            arrive(w_two.at[pl.ds(0, 3)], down_r.at[1])
        advance(chunk, stage)
        for turn, after in enumerate(SHARED):
            if after == (chunk, stage):
                got(normed_copies(turn))
                if turn < 2:
                    go(normed_copies(turn + 1))
                else:
                    shared_expert()
                    sh_in[tp] = sh_part[tp]
        if (chunk, left) == SHARED_SEND_AFTER:
            to_plane(lambda peer: sh_part.at[peer], sh_in.at[tp], sh_s, sh_r)
        if (chunk, left) == (0, -1):
            ret_in[sp] = ret_out[own]

    arrive(sh_in.at[others], sh_r)
    total = hidden[...]
    for j in range(N_TP):
        total = total + sh_in[j].astype(F32)

    for halo in halos:
        halo.wait_send()
    swap.wait_send()
    for ref, send in (
        (mix_w.at[others, pl.ds(0, HEAD // 2)], mix_s),
        (head_all.at[others, rest], head_s),
        (head_all.at[others, first], tail_s),
        (gains.at[others], gain_s),
        (w_one.at[pl.ds(0, 3)], down_s.at[0]),
        (w_two.at[pl.ds(0, 3)], down_s.at[1]),
        (disp_out.at[pl.ds(0, N_SP - 1)], disp_s),
        (sh_in.at[others], sh_s),
    ):
        leave(ref, send)
    kinds = [normed_copies(stage) for stage in range(3)]
    for chunk in range(CHUNKS):
        kinds += [row_copies(chunk, stage) for stage in range(row_stages(chunk))]
        kinds += [expert_copies(chunk, stage) for stage in range(2)]
    for _, ref, index in kinds:
        leave(ref, gat_s.at[index])

    arrive(ret_in.at[pl.ds(0, N_SP - 1)], ret_r)
    returned = ret_in[...].reshape(SLOTS, T)
    total = total + dot(comb_hi[...], returned) + dot(comb_lo[...], returned)
    out[...] = total.T.astype(BF16)
    leave(ret_in.at[pl.ds(0, N_SP - 1)], ret_s)


def local(
    stream,
    values_in,
    in_gate,
    out_gate,
    documents,
    conv_taps,
    head_gain,
    mix_weight,
    norm_gain,
    routes,
    route_weight,
    expert_gate,
    expert_up,
    expert_down,
    shared_gate,
    shared_up,
    shared_down,
):
    vmem = pl.BlockSpec(memory_space=pltpu.VMEM)
    hbm = pl.BlockSpec(memory_space=pl.ANY)
    dma = pltpu.SemaphoreType.DMA
    return pl.pallas_call(
        kernel,
        name="layer",
        out_shape=jax.ShapeDtypeStruct((T, T), BF16),
        in_specs=[hbm] * 17,
        out_specs=vmem,
        scratch_shapes=[
            pltpu.VMEM((T, T), BF16),
            pltpu.VMEM((HEAD, T), BF16),
            pltpu.VMEM((HEAD, T), BF16),
            pltpu.VMEM((HEAD, T), BF16),
            pltpu.VMEM((1, T), jnp.int32),
            pltpu.VMEM((3, HEAD), F32),
            pltpu.VMEM((1, HEAD), F32),
            pltpu.VMEM((1, T), F32),
            pltpu.VMEM((TOP_K, T), jnp.int32),
            pltpu.VMEM((TOP_K, T), F32),
            pltpu.VMEM((HEAD, T), BF16),
            pltpu.VMEM((HEAD, T), BF16),
            pltpu.VMEM((1, T), jnp.int32),
            pltpu.VMEM((HEAD, D), BF16),
            pltpu.VMEM((N_TP, HEAD, T), BF16),
            pltpu.VMEM((D, 2 * T), BF16),
            pltpu.VMEM((SIDE, SIDE, T, T), BF16),
            pltpu.VMEM((SIDE, SIDE, T, T), BF16),
            pltpu.VMEM((SIDE, SIDE, T, T), BF16),
            pltpu.VMEM((D, 2 * T), BF16),
            pltpu.VMEM((T, D), BF16),
            pltpu.VMEM((N_TP, HEAD, T), BF16),
            pltpu.VMEM((N_TP, 1, T), F32),
            pltpu.VMEM((SIDE, SIDE, T, T), BF16),
            pltpu.VMEM((SLOTS, T), BF16),
            pltpu.VMEM((T, SLOTS), BF16),
            pltpu.VMEM((T, SLOTS), BF16),
            pltpu.VMEM((N_SP, CAP, T), BF16),
            pltpu.VMEM((SIDE, SIDE, N_SP, CAP, T), BF16),
            pltpu.VMEM((SIDE, SIDE, N_SP, CAP, T), BF16),
            pltpu.VMEM((SIDE, N_SP, CAP, T), BF16),
            pltpu.VMEM((3, N_SP, CAP, T), BF16),
            pltpu.VMEM((N_SP, CAP, T), BF16),
            pltpu.VMEM((N_SP, CAP, T), BF16),
            pltpu.VMEM((N_TP, T, T), BF16),
            pltpu.VMEM((N_TP, T, T), BF16),
            pltpu.VMEM((T, T), F32),
            pltpu.SemaphoreType.REGULAR((2,)),
            dma((19,)),
            dma((2,)),
            dma((2,)),
            dma((3,)),
            dma((3,)),
            dma,
            dma,
            dma,
            dma,
            dma,
            dma,
            dma,
            dma,
            dma,
            dma,
            dma,
            dma((CHUNKS,)),
            dma((STEPS * CHUNKS + 3,)),
            dma((STEPS * CHUNKS + 3,)),
            dma,
            dma,
            dma,
            dma,
        ],
        compiler_params=pltpu.CompilerParams(collective_id=0, has_side_effects=True),
    )(
        stream,
        values_in,
        in_gate,
        out_gate,
        documents[None, :],
        conv_taps,
        head_gain[None, :],
        mix_weight,
        norm_gain[None, :],
        routes.T,
        route_weight.T,
        expert_gate,
        expert_up,
        expert_down.reshape(SIDE, SIDE, T, T),
        shared_gate,
        shared_up,
        shared_down,
    )


def solution(mesh):
    in_specs = (
        P("tp", "sp"),
        P("tp", "sp"),
        P("tp", "sp"),
        P("tp", "sp"),
        P("sp"),
        P(None, "tp"),
        P("tp"),
        P("tp", None),
        P("tp"),
        P("sp", None),
        P("sp", None),
        P("sp", None, "tp"),
        P("sp", None, "tp"),
        P("sp", None, "tp"),
        P(None, "tp"),
        P(None, "tp"),
        P("tp", None),
    )
    return jax.shard_map(
        local, mesh=mesh, in_specs=in_specs, out_specs=P("tp", "sp"), check_vma=False
    )
```
